32 devices in a mesh: dp: 4 (over y, x), kv: 4 (over z), tp: 2 (over core).
Axes of the slice: x: 2, y: 2, z: 4, core: 2. Of those that a mesh axis runs over, the one named last changes fastest.
Arguments:
- resid: bfloat16 [16, 2048], P('dp', ('kv', 'tp')), may hold values from -45 to 45
- norm_gain: bfloat16 [3, 2048], P(None, ('kv', 'tp')), may hold values from 0.099609375 to 1.8984375
- ffn_gate: bfloat16 [2, 2048, 5632], P(None, None, ('kv', 'tp')), may hold values from -0.125 to 0.125
- ffn_up: bfloat16 [2, 2048, 5632], P(None, None, ('kv', 'tp')), may hold values from -0.125 to 0.125
- ffn_down: bfloat16 [2, 5632, 2048], P(None, ('kv', 'tp')), may hold values from -0.109375 to 0.109375
- w_x: bfloat16 [2048, 64, 64], P(None, 'kv', 'tp'), may hold values from -0.125 to 0.125
- w_z: bfloat16 [2048, 64, 64], P(None, 'kv', 'tp'), may hold values from -0.125 to 0.125
- w_bc: bfloat16 [2048, 2, 8, 128], P('kv'), may hold values from -0.125 to 0.125
- w_dt: bfloat16 [2048, 64], P('kv'), may hold values from -0.125 to 0.125
- dt_bias: float32 [64], replicated, may hold values from -2 to 0.5
- a_log: float32 [64], replicated, may hold values from -1.5 to 1.5
- d_skip: float32 [64], replicated, may hold values from 0.5 to 1.5
- conv_wx: bfloat16 [4, 64, 64], P(None, None, 'tp'), may hold values from -3 to 3
- conv_wbc: bfloat16 [4, 2, 8, 128], replicated, may hold values from -3 to 3
- conv_x: bfloat16 [16, 3, 64, 64], P(('dp', 'kv'), None, None, 'tp'), may hold values from -6 to 6
- conv_bc: bfloat16 [16, 3, 2, 8, 128], P(('dp', 'kv')), may hold values from -6 to 6
- ssm_state: float32 [16, 64, 64, 128], P(('dp', 'kv'), None, 'tp'), may hold values from -3 to 3
- w_out: bfloat16 [64, 64, 2048], P(None, 'tp', 'kv'), may hold values from -0.09375 to 0.09375
Outputs:
- final: bfloat16 [16, 2048], P('dp', ('kv', 'tp'))
The draws below stay inside these ranges and needn't reach their ends.
All inputs are finite; a program needn't handle non-finite values.
Results may differ from the reference program's by a relative error of at most 0.018.
Values may be sent and summed in bfloat16 or wider, within the bound.
No kernel may reach another device: no remote copies, remote signals or barrier semaphores. Data moves between devices by JAX's collectives and lax.ppermute only.
A program may use at most 64 MiB of HBM per device.

```python
import math
import jax
import jax.numpy as jnp
from jax import lax

D = 2048
FF = 5632
H = 64
P_SIZE = 64
G = 8
STATE = 128
CONV = 4
SEQ_DEV = 1
BATCH = 16


def draw_resid(key, part):
    first_key = jax.random.fold_in(key, 11)
    second_key = jax.random.fold_in(key, 12)
    third_key = jax.random.fold_in(key, 13)
    columns = jnp.arange(D, dtype=jnp.float32) / D
    col_scale = 0.4 * jnp.exp(jnp.log(6.0) * columns) * jax.random.uniform(second_key, (D,), jnp.float32, 0.5, 1.5)
    row_scale = 0.3 * jnp.exp(jax.random.uniform(third_key, (BATCH, 1), jnp.float32, 0.0, jnp.log(10.0)))
    base = jnp.clip(jax.random.normal(first_key, (BATCH, D), jnp.float32), -4.0, 4.0)
    return (base * col_scale[None, :] * row_scale).astype(jnp.bfloat16)


def strengthened(result, stream_key, source, target, parts, factor):
    def block_of(axis_at):
        return (jnp.arange(result.shape[axis_at]) // (result.shape[axis_at] // parts)).reshape((-1,) + (1,) * (result.ndim - 1 - axis_at))

    near = jax.random.permutation(stream_key, parts)[block_of(target)]
    other_side = (block_of(target) + parts // 2) % parts
    return jnp.where((block_of(source) == near) | (block_of(source) == other_side), factor * result, result)


def steps_of(key, dims, split, low, largest):
    level, own = 1.0, jax.random.fold_in(key, 6)
    for dim, parts in split:
        heights = jnp.exp(jax.random.uniform(jax.random.fold_in(own, dim), (parts,), jnp.float32, low / len(split), largest / len(split)))
        level = level * jnp.repeat(heights, dims[dim] // parts).reshape([-1 if axis == dim else 1 for axis in range(len(dims))])
    return level


def noise(own_key, extent, spread, bound, pieces=(), held_as=jnp.bfloat16):
    values = jax.random.normal(own_key, extent, jnp.float32) * spread
    if len(pieces) > 0:
        values = steps_of(own_key, extent, pieces, -0.22, 0.18) * values
    return jnp.clip(values, min=-bound, max=bound).astype(held_as)


def bell_draw_with(stream_key, shape, deviation, reach, pieces, heavy, held_as=jnp.bfloat16):
    values = deviation * jax.random.normal(stream_key, shape, jnp.float32)
    if pieces:
        values = values * steps_of(stream_key, shape, pieces, -0.22, 0.18)
    return jnp.clip(strengthened(values, jax.random.fold_in(stream_key, 3), *heavy), -reach, reach).astype(held_as)


def setup_inputs(seed: int = 0) -> dict:
    key_list = jax.random.split(jax.random.key(seed), 19)
    return {
        "resid": draw_resid(jax.random.fold_in(key_list[18], 71), 0),
        "norm_gain": jnp.clip(1.0 + 0.18 * jax.random.normal(key_list[1], (3, D), jnp.float32), 0.099609375, 1.8984375).astype(jnp.bfloat16),
        "ffn_gate": noise(key_list[2], (2, D, FF), D ** -0.5, 0.125, ((2, 8),)),
        "ffn_up": noise(key_list[3], (2, D, FF), D ** -0.5, 0.125, ((2, 8),)),
        "ffn_down": bell_draw_with(key_list[4], (2, FF, D), FF ** -0.5, 0.109375, ((1, 8),), (1, 2, 8, 2.0)),
        "w_x": noise(key_list[5], (D, H, P_SIZE), D ** -0.5, 0.125, ((1, 4), (2, 2))),
        "w_z": noise(key_list[6], (D, H, P_SIZE), D ** -0.5, 0.125, ((1, 4), (2, 2))),
        "w_bc": noise(key_list[7], (D, 2, G, STATE), D ** -0.5, 0.125, ((0, 4),)),
        "w_dt": noise(key_list[8], (D, H), D ** -0.5, 0.125, ((0, 4),)),
        "dt_bias": jnp.clip(jax.random.uniform(key_list[9], (H,), jnp.float32, -2.0, 0.5), -2.0, 0.5),
        "a_log": jnp.clip(jax.random.uniform(key_list[10], (H,), jnp.float32, -1.5, 1.5), -1.5, 1.5),
        "d_skip": jnp.clip(jnp.exp(jax.random.uniform(key_list[11], (H,), jnp.float32, math.log(0.5), math.log(1.5))), 0.5, 1.5),
        "conv_wx": noise(key_list[12], (CONV, H, P_SIZE), CONV ** -0.5, 3.0, ((2, 2),)),
        "conv_wbc": noise(key_list[13], (CONV, 2, G, STATE), CONV ** -0.5, 3.0),
        "conv_x": noise(key_list[14], (BATCH, CONV - 1, H, P_SIZE), 1.0, 6.0, ((0, 16), (3, 2))),
        "conv_bc": noise(key_list[15], (BATCH, CONV - 1, 2, G, STATE), 1.0, 6.0, ((0, 16),)),
        "ssm_state": noise(key_list[16], (BATCH, H, P_SIZE, STATE), 0.3, 3.0, ((0, 16), (2, 2)), jnp.float32),
        "w_out": noise(key_list[17], (H, P_SIZE, D), (H * P_SIZE) ** -0.5, 0.09375, ((1, 2), (2, 4))),
    }


EPS = 1e-06

def normalize(rows, gain):
    values = rows.astype(jnp.float32)
    scale = lax.rsqrt(lax.optimization_barrier(jnp.mean(values * values, axis=1, keepdims=True)) + EPS)
    return (values * scale * gain.astype(jnp.float32)[None, :]).astype(jnp.bfloat16)

def feed_forward(normed, w_gate, w_up, w_down):
    gate = jnp.dot(normed, w_gate, preferred_element_type=jnp.float32)
    upper = jnp.dot(normed, w_up, preferred_element_type=jnp.float32)
    hidden = (jax.nn.silu(gate) * upper).astype(jnp.bfloat16)
    return jnp.dot(hidden, w_down, preferred_element_type=jnp.float32)

def short_conv(history, newest, taps):
    window = jnp.concatenate([history.astype(jnp.float32), newest.astype(jnp.float32)[:, None]], axis=1)
    return jax.nn.silu(lax.optimization_barrier(jnp.sum(window * taps.astype(jnp.float32)[None], axis=1)))

def state_step(xs_new, zeta, bc_new, dt_raw, conv_x, conv_bc, ssm_state, conv_wx, conv_wbc, dt_bias, a_log, d_skip):
    xconv = short_conv(conv_x, xs_new, conv_wx)
    bconv = short_conv(conv_bc, bc_new, conv_wbc)
    heads = xconv.shape[1]
    groups = bconv.shape[2]
    bmat = jnp.repeat(bconv[:, 0], heads // groups, axis=1)
    cmat = jnp.repeat(bconv[:, 1], heads // groups, axis=1)
    step_size = jax.nn.softplus(dt_raw + dt_bias[None, :])
    decay = jnp.exp(-step_size * jnp.exp(a_log)[None, :])
    updated = decay[:, :, None, None] * ssm_state + (step_size[:, :, None] * xconv)[..., None] * bmat[:, :, None, :]
    mixed = jnp.einsum('shpn,shn->shp', updated, cmat, precision=lax.Precision.HIGHEST) + d_skip[None, :, None] * xconv
    return (mixed * jax.nn.silu(zeta.astype(jnp.float32))).astype(jnp.bfloat16)

def reference(resid, norm_gain, ffn_gate, ffn_up, ffn_down, w_x, w_z, w_bc, w_dt, dt_bias, a_log, d_skip, conv_wx, conv_wbc, conv_x, conv_bc, ssm_state, w_out):
    total = resid.shape[0]
    heads = w_x.shape[1]
    channels = w_x.shape[2]
    normed = normalize(resid, norm_gain[0])
    first = (resid.astype(jnp.float32) + 0.5 * feed_forward(normed, ffn_gate[0], ffn_up[0], ffn_down[0])).astype(jnp.bfloat16)
    normed = normalize(first, norm_gain[1])
    xs_new = jnp.dot(normed, w_x.reshape(D, -1), preferred_element_type=jnp.float32).astype(jnp.bfloat16).reshape(total, heads, channels)
    zeta = jnp.dot(normed, w_z.reshape(D, -1), preferred_element_type=jnp.float32).astype(jnp.bfloat16).reshape(total, heads, channels)
    bc_new = jnp.dot(normed, w_bc.reshape(D, -1), preferred_element_type=jnp.float32).astype(jnp.bfloat16).reshape((total,) + w_bc.shape[1:])
    dt_raw = jnp.dot(normed, w_dt, preferred_element_type=jnp.float32)
    blocks = total // SEQ_DEV

    def fold(values):
        return values.reshape((blocks, SEQ_DEV) + values.shape[1:])

    def per_block(items):
        return state_step(*items, conv_wx, conv_wbc, dt_bias, a_log, d_skip)
    outputs = lax.map(per_block, (fold(xs_new), fold(zeta), fold(bc_new), fold(dt_raw), fold(conv_x), fold(conv_bc), fold(ssm_state)))
    outputs = outputs.reshape(total, heads * channels)
    second = (first.astype(jnp.float32) + jnp.dot(outputs, w_out.reshape(heads * channels, D), preferred_element_type=jnp.float32)).astype(jnp.bfloat16)
    normed = normalize(second, norm_gain[2])
    final = second.astype(jnp.float32) + 0.5 * feed_forward(normed, ffn_gate[1], ffn_up[1], ffn_down[1])
    return final.astype(jnp.bfloat16)
```

```python
import functools

import jax
import jax.numpy as jnp
from jax import lax
from jax.experimental import pallas as pl
from jax.experimental.pallas import tpu as pltpu
from jax.sharding import PartitionSpec as P

EPS = 1e-06
F32 = jnp.float32
BF16 = jnp.bfloat16
NT = (((1,), (1,)), ((), ()))
ANY = pl.BlockSpec(memory_space=pl.ANY)
VMEM = pl.BlockSpec(memory_space=pltpu.VMEM)


def dot_nt(left, right):
    return lax.dot_general(left, right, NT, preferred_element_type=F32)


def dot_nn(left, right):
    return jnp.dot(left, right, preferred_element_type=F32)


def silu(value):
    return value * jax.nn.sigmoid(value)


def swap_kv(value, kv, distance):
    return lax.ppermute(value, "kv", [(i, i ^ distance) for i in range(kv)])


def swap_tp(value):
    return lax.ppermute(value, "tp", [(0, 1), (1, 0)])


def share_kv(value, kv):
    return [value] + [swap_kv(value, kv, d) for d in range(1, kv)]


def in_vmem(value):
    return pltpu.with_memory_space_constraint(value, pltpu.VMEM)


def run(body, outs, args, scratch=(), limit=16, in_specs=None, name=None, flops=0):
    return pl.pallas_call(
        body,
        out_shape=outs,
        in_specs=in_specs or [VMEM] * len(args),
        out_specs=jax.tree.map(lambda _: VMEM, outs),
        scratch_shapes=list(scratch),
        compiler_params=pltpu.CompilerParams(vmem_limit_bytes=limit * 2**20),
        cost_estimate=pl.CostEstimate(flops=flops, bytes_accessed=0, transcendentals=0),
        name=name,
    )(*args)


def f32(*shape):
    return jax.ShapeDtypeStruct(shape, F32)


def bf16(*shape):
    return jax.ShapeDtypeStruct(shape, BF16)


def fetch_ffn_body(layer, gate, up, down, gate_out, up_out, down_out, sems):
    copies = [
        pltpu.make_async_copy(source.at[layer], target, sems.at[i])
        for i, (source, target) in enumerate(
            ((gate, gate_out), (up, up_out), (down, down_out))
        )
    ]
    for copy in copies:
        copy.start()
    for copy in copies:
        copy.wait()


def fetch_ffn(layer, gate, up, down):
    outs = [pltpu.VMEM(a.shape[1:], a.dtype) for a in (gate, up, down)]
    return run(
        functools.partial(fetch_ffn_body, layer),
        outs,
        (gate, up, down),
        [pltpu.SemaphoreType.DMA((3,))],
        4,
        [ANY] * 3,
        f"fetch_ffn_{layer}",
        flops=10**7,
    )


def fetch_mix_body(w_x, w_z, w_bc, w_dt, w_out, state, xz_out, bc_out, dt_out, out_out, high_out, low_out, held, sems):
    width = w_x.shape[0]
    pairs = (
        (state, held),
        (w_x, xz_out.at[pl.ds(0, width)]),
        (w_z, xz_out.at[pl.ds(width, width)]),
        (w_bc, bc_out),
        (w_dt, dt_out),
        (w_out, out_out),
    )
    copies = [pltpu.make_async_copy(a, b, sems.at[i]) for i, (a, b) in enumerate(pairs)]
    for copy in copies:
        copy.start()
    copies[0].wait()
    values = held[...]
    high = values.astype(BF16)
    high_out[...] = high
    low_out[...] = (values - high.astype(F32)).astype(BF16)
    for copy in copies[1:]:
        copy.wait()


def fetch_mix(w_x, w_z, w_bc, w_dt, w_out, state):
    outs = [
        pltpu.VMEM((2 * w_x.shape[0], w_x.shape[1]), BF16),
        pltpu.VMEM(w_bc.shape, BF16),
        pltpu.VMEM(w_dt.shape, BF16),
        pltpu.VMEM(w_out.shape, BF16),
        pltpu.VMEM(state.shape, BF16),
        pltpu.VMEM(state.shape, BF16),
    ]
    return run(
        fetch_mix_body,
        outs,
        (w_x, w_z, w_bc, w_dt, w_out, state),
        [pltpu.VMEM(state.shape, F32), pltpu.SemaphoreType.DMA((6,))],
        8,
        [ANY] * 6,
        "fetch_mix",
        flops=10**7,
    )


def normed_rows(values, gain):
    scale = lax.rsqrt(jnp.mean(values * values, axis=1, keepdims=True) + EPS)
    return (values * scale * gain).astype(BF16)


def feed(normed, gate, up, down):
    hidden = (silu(dot_nt(normed, gate[...])) * dot_nt(normed, up[...])).astype(BF16)
    return dot_nn(hidden, down[...])


def first_body(kv, seqs, own, other, gate, up, down, sums_out, rows_out, slabs):
    here, side = lax.axis_index("kv"), lax.axis_index("tp")
    width = slabs.shape[2]
    for d in range(kv):
        peer = jnp.bitwise_xor(here, d)
        slabs[2 * peer + side] = own[:, d * width : (d + 1) * width]
        slabs[2 * peer + 1 - side] = other[:, d * width : (d + 1) * width]
    rows = jnp.concatenate([slabs[i] for i in range(slabs.shape[0])], axis=1)
    rows_out[...] = rows
    values = rows.astype(F32)
    sums = feed(normed_rows(values, values[seqs : seqs + 1]), gate, up, down)
    sums_out[...] = sums[:seqs]


def mix_in_body(kv, seqs, s0, s1, s2, s3, rows, w_xz, w_bc, w_dt, *rest):
    pays, (first_out, slabs, firsts, table) = rest[:kv], rest[kv:]
    here = lax.axis_index("kv")
    span = slabs.shape[2]
    total = s0[...].astype(F32) + s1[...].astype(F32) + s2[...].astype(F32) + s3[...].astype(F32)
    known = rows[...].astype(F32)
    first = (known[:seqs] + 0.5 * total).astype(BF16).astype(F32)
    padded = jnp.concatenate([first, first], axis=0)
    normed = normed_rows(padded, known[seqs + 1 : seqs + 2])
    for i in range(kv):
        slabs[i] = normed[:, i * span : (i + 1) * span].astype(F32)
        firsts[i] = padded[:, i * span : (i + 1) * span]
    slab = slabs[here].astype(BF16)
    first_out[...] = firsts[here][:seqs]
    xz = dot_nt(normed, w_xz[...]).astype(BF16).astype(F32)
    bc = dot_nn(slab, w_bc[...])
    dt = dot_nt(slab, w_dt[...])
    a = xz.shape[1]
    b = a + bc.shape[1]
    table[:, :a] = xz
    table[:, a:b] = bc
    table[:, b : b + dt.shape[1]] = dt
    for d in range(kv):
        pays[d][...] = table[pl.ds(jnp.bitwise_xor(here, d), 1), :]


def state_body(kv, p0, p1, p2, p3, high, low, taps_x, past_x, taps_bc, past_bc, bias, a_log, d_skip, out, x_held, z_held, bc_held):
    here = lax.axis_index("kv")
    groups, wide = x_held.shape
    states = bc_held.shape[1]
    heads = bias.shape[1]
    pieces = (p0, p1, p2, p3)
    per = groups // kv
    width = per * wide
    for d, piece in enumerate(pieces):
        peer = jnp.bitwise_xor(here, d)
        for i in range(per):
            x_held[pl.ds(per * peer + i, 1), :] = piece[:, i * wide : (i + 1) * wide]
            z_held[pl.ds(per * peer + i, 1), :] = piece[:, width + i * wide : width + (i + 1) * wide]
    a = 2 * width
    for j in range(2 * groups):
        at = a + j * states
        bc_held[j : j + 1, :] = sum(piece[:, at : at + states] for piece in pieces)
    b = a + 2 * groups * states
    dt = sum(piece[:, b : b + heads] for piece in pieces) + bias[...]
    newest = bc_held[...].astype(BF16).astype(F32)
    steps = taps_bc.shape[0]
    mapped = newest * taps_bc[steps - 1].astype(F32)
    for k in range(steps - 1):
        mapped += past_bc[k].astype(F32) * taps_bc[k].astype(F32)
    mapped = silu(mapped)
    b_map, c_map = mapped[:groups], mapped[groups:]
    xconv = x_held[...] * taps_x[steps - 1].astype(F32)
    for k in range(steps - 1):
        xconv += past_x[k].astype(F32) * taps_x[k].astype(F32)
    xconv = silu(xconv)
    share = heads // groups
    own_group = lax.broadcasted_iota(jnp.int32, (groups, heads), 1) // share == lax.broadcasted_iota(
        jnp.int32, (groups, heads), 0
    )
    spread = (
        lax.broadcasted_iota(jnp.int32, (heads, wide), 0) % share
        == lax.broadcasted_iota(jnp.int32, (heads, wide), 1) // (wide // share)
    ).astype(F32)
    table = jnp.concatenate(
        [
            jnp.where(own_group, jnp.broadcast_to(v, (groups, heads)), 0.0)
            for v in (dt, a_log[...], d_skip[...])
        ],
        axis=0,
    )
    table = jnp.dot(table, spread, precision=lax.Precision.HIGHEST, preferred_element_type=F32)
    step = jax.nn.softplus(table[:groups])
    decay = jnp.exp(-step * jnp.exp(table[groups : 2 * groups]))
    skip = table[2 * groups :]
    c_high = c_map.astype(BF16)
    c_low = (c_map - c_high.astype(F32)).astype(BF16)
    read = dot_nt(c_high, high[...]) + dot_nt(c_low, high[...]) + dot_nt(c_high, low[...])
    read = jnp.concatenate(
        [read[g : g + 1, g * wide : (g + 1) * wide] for g in range(groups)], axis=0
    )
    inner = jnp.sum(b_map * c_map, axis=1, keepdims=True)
    mixed = (decay * read + xconv * (step * inner + skip)) * silu(z_held[...])
    mixed = mixed.astype(BF16).astype(F32)
    for g in range(groups):
        out[:, g * wide : (g + 1) * wide] = mixed[g : g + 1]


def mix_out_body(kv, seqs, tp, m0, m1, m2, m3, w_out, first, out, table):
    here = lax.axis_index("kv")
    table[...] = jnp.zeros_like(table)
    for d, piece in enumerate((m0, m1, m2, m3)):
        table[pl.ds(jnp.bitwise_xor(here, d), 1), :] = piece[...]
    sums = dot_nn(table[...].astype(BF16), w_out[...])
    out[...] = sums[:seqs] + first[...] * (1.0 / tp)


def second_body(kv, seqs, s0, s1, s2, s3, rows, gate, up, down, *rest):
    outs, (own_out, slabs, sums_held) = rest[:kv], rest[kv:]
    here = lax.axis_index("kv")
    span = slabs.shape[2]
    for d, piece in enumerate((s0, s1, s2, s3)):
        slabs[jnp.bitwise_xor(here, d)] = piece[...].astype(F32)
    second = jnp.concatenate([slabs[i] for i in range(kv)], axis=1)
    padded = jnp.concatenate([second, second], axis=0)
    gain = rows[seqs + 2 : seqs + 3, :].astype(F32)
    sums = feed(normed_rows(padded, gain), gate, up, down)[:seqs]
    for i in range(kv):
        sums_held[i] = sums[:, i * span : (i + 1) * span]
    for d in range(kv):
        outs[d][...] = sums_held[jnp.bitwise_xor(here, d)]
    own_out[...] = s0[...].astype(F32)


def small_mesh(
    kv,
    tp,
    resid,
    norm_gain,
    ffn_gate,
    ffn_up,
    ffn_down,
    w_x,
    w_z,
    w_bc,
    w_dt,
    dt_bias,
    a_log,
    d_skip,
    conv_wx,
    conv_wbc,
    conv_x,
    conv_bc,
    ssm_state,
    w_out,
):
    seqs, width = resid.shape
    model = width * kv * tp
    span = model // kv
    gate, up = jnp.swapaxes(ffn_gate, 1, 2), jnp.swapaxes(ffn_up, 1, 2)
    units = gate.shape[1]
    heads = dt_bias.shape[0]
    groups, states = w_bc.shape[2:]
    half = w_x.shape[2]
    local = w_x.shape[1] * half
    wide = heads // groups * half
    flat = heads * half

    pack = jnp.concatenate([resid, norm_gain, norm_gain[:1]], axis=0)
    chip = jnp.concatenate(share_kv(pack, kv), axis=1)
    other = swap_tp(chip)
    weights_one = fetch_ffn(0, gate, up, ffn_down)
    sums, rows = run(
        functools.partial(first_body, kv, seqs),
        [f32(seqs, model), bf16(2 * seqs, model)],
        (chip, other, *map(in_vmem, weights_one)),
        [pltpu.VMEM((kv * tp, 2 * seqs, width), BF16)],
        name="first_ffn",
    )
    sums = (sums + swap_tp(sums)).astype(BF16)
    sums = share_kv(sums, kv)

    mix_weights = fetch_mix(
        jnp.transpose(w_x, (1, 2, 0)).reshape(local, model),
        jnp.transpose(w_z, (1, 2, 0)).reshape(local, model),
        w_bc.reshape(span, 2 * groups * states),
        w_dt.T,
        w_out.reshape(flat, span),
        ssm_state.reshape(flat, states),
    )
    w_xz, w_maps, w_steps, w_join, high, low = map(in_vmem, mix_weights)
    bc_width = 2 * groups * states
    line = 2 * local + bc_width + max(heads, 128)
    *pays, first = run(
        functools.partial(mix_in_body, kv, seqs),
        [f32(1, line)] * kv + [f32(seqs, span)],
        (*sums, rows, w_xz, w_maps, w_steps),
        [
            pltpu.VMEM((kv, 2 * seqs, span), F32),
            pltpu.VMEM((kv, 2 * seqs, span), F32),
            pltpu.VMEM((2 * seqs, line), F32),
        ],
        name="mix_in",
    )
    pays = pays[:1] + [swap_kv(pays[d], kv, d) for d in range(1, kv)]
    mixed = run(
        functools.partial(state_body, kv),
        f32(1, flat),
        (
            *pays,
            high,
            low,
            conv_wx.reshape(-1, groups, wide),
            conv_x.reshape(-1, groups, wide),
            conv_wbc.reshape(-1, 2 * groups, states),
            conv_bc.reshape(-1, 2 * groups, states),
            dt_bias.reshape(1, heads),
            a_log.reshape(1, heads),
            d_skip.reshape(1, heads),
        ),
        [
            pltpu.VMEM((groups, wide), F32),
            pltpu.VMEM((groups, wide), F32),
            pltpu.VMEM((2 * groups, states), F32),
        ],
        name="state_step",
    )
    mixed = share_kv(mixed, kv)
    joined = run(
        functools.partial(mix_out_body, kv, seqs, tp),
        f32(seqs, span),
        (*mixed, w_join, first),
        [pltpu.VMEM((2 * seqs, flat), F32)],
        name="mix_out",
    )
    second = share_kv((joined + swap_tp(joined)).astype(BF16), kv)
    weights_two = fetch_ffn(1, gate, up, ffn_down)
    *sums, own = run(
        functools.partial(second_body, kv, seqs),
        [f32(seqs, span)] * kv + [f32(seqs, span)],
        (*second, rows, *map(in_vmem, weights_two)),
        [pltpu.VMEM((kv, seqs, span), F32), pltpu.VMEM((kv, seqs, span), F32)],
        name="second_ffn",
    )
    total = sums[0] + sum(swap_kv(sums[d], kv, d) for d in range(1, kv))
    side = lax.axis_index("tp")
    mine = lax.dynamic_slice_in_dim(total, side * width, width, 1)
    theirs = lax.dynamic_slice_in_dim(total, (1 - side) * width, width, 1)
    base = lax.dynamic_slice_in_dim(own, side * width, width, 1)
    return (base + 0.5 * (mine + swap_tp(theirs))).astype(BF16)


def normalize(rows, gain):
    values = rows.astype(jnp.float32)
    scale = lax.rsqrt(jnp.mean(values * values, axis=1, keepdims=True) + EPS)
    return (values * scale * gain.astype(jnp.float32).reshape(1, -1)).astype(jnp.bfloat16)


def feed_forward(normed, w_gate, w_up, w_down):
    gate = jnp.dot(normed, w_gate, preferred_element_type=jnp.float32)
    upper = jnp.dot(normed, w_up, preferred_element_type=jnp.float32)
    hidden = (jax.nn.silu(gate) * upper).astype(jnp.bfloat16)
    return jnp.dot(hidden, w_down, preferred_element_type=jnp.float32)


def add_half(base, sums):
    return (base.astype(jnp.float32) + 0.5 * sums).astype(jnp.bfloat16)


def ffn_totals(partial_value):
    return lax.psum(partial_value, ("kv", "tp"))


def short_conv(history, newest, taps):
    window = jnp.concatenate(
        [history.astype(jnp.float32), newest.astype(jnp.float32)[:, None]], axis=1
    )
    return jax.nn.silu(jnp.sum(window * taps.astype(jnp.float32)[None], axis=1))


def state_step(
    xs_new,
    zeta,
    bc_new,
    dt_raw,
    conv_x,
    conv_bc,
    ssm_state,
    conv_wx,
    conv_wbc,
    dt_bias,
    a_log,
    d_skip,
):
    xconv = short_conv(conv_x, xs_new, conv_wx)
    bconv = short_conv(conv_bc, bc_new, conv_wbc)
    heads = xconv.shape[1]
    groups = bconv.shape[2]
    bmat = jnp.repeat(bconv[:, 0], heads // groups, axis=1)
    cmat = jnp.repeat(bconv[:, 1], heads // groups, axis=1)
    step_size = jax.nn.softplus(dt_raw + dt_bias[None, :])
    decay = jnp.exp(-step_size * jnp.exp(a_log)[None, :])
    updated = (
        decay[:, :, None, None] * ssm_state
        + (step_size[:, :, None] * xconv)[..., None] * bmat[:, :, None, :]
    )
    mixed = (
        jnp.einsum("shpn,shn->shp", updated, cmat, precision=lax.Precision.HIGHEST)
        + d_skip[None, :, None] * xconv
    )
    return (mixed * jax.nn.silu(zeta.astype(jnp.float32))).astype(jnp.bfloat16)


def group_terms(slab, w_bc, w_dt):
    span = slab.shape[1]
    flat_bc = w_bc.reshape(span, -1)
    bc_part = jnp.dot(slab, flat_bc, preferred_element_type=jnp.float32)
    dt_part = jnp.dot(slab, w_dt, preferred_element_type=jnp.float32)
    return (
        lax.psum_scatter(bc_part, "kv", scatter_dimension=0, tiled=True),
        lax.psum_scatter(dt_part, "kv", scatter_dimension=0, tiled=True),
    )


def mix_partial(
    normed,
    w_x,
    w_z,
    w_bc,
    w_dt,
    dt_bias,
    a_log,
    d_skip,
    conv_wx,
    conv_wbc,
    conv_x,
    conv_bc,
    ssm_state,
    w_out,
):
    rows = normed.shape[0]
    local_heads = w_x.shape[1]
    half = w_x.shape[2]
    xs_part = (
        jnp.dot(normed, w_x.reshape(normed.shape[1], -1), preferred_element_type=jnp.float32)
        .astype(jnp.bfloat16)
        .reshape(rows, local_heads, half)
    )
    zeta_part = (
        jnp.dot(normed, w_z.reshape(normed.shape[1], -1), preferred_element_type=jnp.float32)
        .astype(jnp.bfloat16)
        .reshape(rows, local_heads, half)
    )
    xs_new, zeta = (
        lax.all_to_all(xs_part, "kv", split_axis=0, concat_axis=1, tiled=True),
        lax.all_to_all(zeta_part, "kv", split_axis=0, concat_axis=1, tiled=True),
    )
    span = w_bc.shape[0]
    slab = lax.dynamic_slice_in_dim(normed, lax.axis_index("kv") * span, span, 1)
    bc_sum, dt_raw = group_terms(slab, w_bc, w_dt)
    bc_new = bc_sum.astype(jnp.bfloat16).reshape((bc_sum.shape[0],) + w_bc.shape[1:])
    mixed = state_step(
        xs_new,
        zeta,
        bc_new,
        dt_raw,
        conv_x,
        conv_bc,
        ssm_state,
        conv_wx,
        conv_wbc,
        dt_bias,
        a_log,
        d_skip,
    )
    flat_out = w_out.reshape(-1, w_out.shape[2])
    piece = lax.all_gather(mixed, "kv", axis=0, tiled=True)
    return jnp.dot(piece.reshape(piece.shape[0], -1), flat_out, preferred_element_type=jnp.float32)


def per_device(
    resid,
    norm_gain,
    ffn_gate,
    ffn_up,
    ffn_down,
    w_x,
    w_z,
    w_bc,
    w_dt,
    dt_bias,
    a_log,
    d_skip,
    conv_wx,
    conv_wbc,
    conv_x,
    conv_bc,
    ssm_state,
    w_out,
):
    mixer_args = (
        w_x,
        w_z,
        w_bc,
        w_dt,
        dt_bias,
        a_log,
        d_skip,
        conv_wx,
        conv_wbc,
        conv_x,
        conv_bc,
        ssm_state,
        w_out,
    )
    rows, gains = (
        lax.all_gather(resid, ("kv", "tp"), axis=1, tiled=True),
        lax.all_gather(norm_gain, ("kv", "tp"), axis=1, tiled=True),
    )
    first = add_half(
        rows,
        ffn_totals(feed_forward(normalize(rows, gains[0]), ffn_gate[0], ffn_up[0], ffn_down[0])),
    )
    partial_value = mix_partial(normalize(first, gains[1]), *mixer_args)
    span = partial_value.shape[1]
    block = lax.dynamic_slice_in_dim(first, lax.axis_index("kv") * span, span, 1)
    joined = (block.astype(jnp.float32) + lax.psum(partial_value, "tp")).astype(jnp.bfloat16)
    second = lax.all_gather(joined, "kv", axis=1, tiled=True)
    final = add_half(
        second,
        ffn_totals(feed_forward(normalize(second, gains[2]), ffn_gate[1], ffn_up[1], ffn_down[1])),
    )
    width = resid.shape[1]
    return lax.dynamic_slice_in_dim(final, lax.axis_index(("kv", "tp")) * width, width, 1)


def solution(mesh):
    placed = (
        P("dp", ("kv", "tp")),
        P(None, ("kv", "tp")),
        P(None, None, ("kv", "tp")),
        P(None, None, ("kv", "tp")),
        P(None, ("kv", "tp"), None),
        P(None, "kv", "tp"),
        P(None, "kv", "tp"),
        P("kv", None, None, None),
        P("kv", None),
        P(),
        P(),
        P(),
        P(None, None, "tp"),
        P(),
        P(("dp", "kv"), None, None, "tp"),
        P(("dp", "kv"), None, None, None, None),
        P(("dp", "kv"), None, "tp", None),
        P(None, "tp", "kv"),
    )
    kv, tp = mesh.shape["kv"], mesh.shape["tp"]
    step = functools.partial(small_mesh, kv, tp) if (kv, tp) == (4, 2) else per_device
    return jax.shard_map(
        step, mesh=mesh, in_specs=placed, out_specs=P("dp", ("kv", "tp")), check_vma=False
    )
```

```python
import functools

import jax
import jax.numpy as jnp
from jax import lax
from jax.experimental import pallas as pl
from jax.experimental.pallas import tpu as pltpu
from jax.sharding import PartitionSpec as P


EPS = 1e-06
F32 = jnp.float32
BF16 = jnp.bfloat16
NT = (((1,), (1,)), ((), ()))
ANY = pl.BlockSpec(memory_space=pl.ANY)
VMEM = pl.BlockSpec(memory_space=pltpu.VMEM)


def dot_nt(left, right):
    return lax.dot_general(left, right, NT, preferred_element_type=F32)


def dot_nn(left, right):
    return jnp.dot(left, right, preferred_element_type=F32)


def silu(value):
    return value * jax.nn.sigmoid(value)


def swap_kv(values):
    kv = len(values)
    got = list(values)
    for d in reversed(range(1, kv)):
        got[d] = lax.ppermute(values[d], "kv", [(i, i ^ d) for i in range(kv)])
    return got


def share_kv(value, kv):
    return swap_kv([value] * kv)


def swap_tp(value):
    return lax.ppermute(value, "tp", [(0, 1), (1, 0)])


def in_vmem(value):
    return pltpu.with_memory_space_constraint(value, pltpu.VMEM)


def run(body, outs, args, scratch=(), limit=16, in_specs=None, flops=10**10):
    return pl.pallas_call(
        body,
        out_shape=outs,
        in_specs=in_specs or [VMEM] * len(args),
        out_specs=jax.tree.map(lambda _: VMEM, outs),
        scratch_shapes=list(scratch),
        compiler_params=pltpu.CompilerParams(vmem_limit_bytes=limit * 2**20),
        cost_estimate=pl.CostEstimate(flops=flops, bytes_accessed=0, transcendentals=0),
    )(*args)


def f32(*shape):
    return jax.ShapeDtypeStruct(shape, F32)


def bf16(*shape):
    return jax.ShapeDtypeStruct(shape, BF16)


def split_body(state, high_out, low_out):
    values = state[...]
    high = values.astype(BF16)
    high_out[...] = high
    low_out[...] = (values - high.astype(F32)).astype(BF16)


def normed_rows(values, gain):
    scale = lax.rsqrt(jnp.mean(values * values, axis=1, keepdims=True) + EPS)
    return (values * scale * gain).astype(BF16)


def feed(normed, layer, gate, up, down):
    hidden = (silu(dot_nt(normed, gate[layer])) * dot_nt(normed, up[layer])).astype(BF16)
    return dot_nn(hidden, down[layer])


def pack_body(rows, gains, out):
    seqs = rows.shape[0]
    out[:seqs] = rows[...]
    out[seqs : seqs + gains.shape[0]] = gains[...]
    out[seqs + gains.shape[0] :] = gains[:1]


def first_body(kv, seqs, own, other, gate, up, down, sums_out, rows_out, slabs):
    here, side = lax.axis_index("kv"), lax.axis_index("tp")
    width = slabs.shape[2]
    for d in range(kv):
        peer = jnp.bitwise_xor(here, d)
        slabs[2 * peer + side] = own[:, d * width : (d + 1) * width]
        slabs[2 * peer + 1 - side] = other[:, d * width : (d + 1) * width]
    rows = jnp.concatenate([slabs[i] for i in range(slabs.shape[0])], axis=1)
    rows_out[...] = rows
    values = rows.astype(F32)
    sums = feed(normed_rows(values, values[seqs : seqs + 1]), 0, gate, up, down)
    sums_out[...] = sums[:seqs]


def mix_in_body(kv, seqs, s0, s1, s2, s3, rows, w_x, w_z, w_bc, w_dt, *rest):
    pays, (first_out, slabs, firsts, table) = rest[:kv], rest[kv:]
    here = lax.axis_index("kv")
    span = slabs.shape[2]
    total = s0[...].astype(F32) + s1[...].astype(F32) + s2[...].astype(F32) + s3[...].astype(F32)
    known = rows[...].astype(F32)
    first = (known[:seqs] + 0.5 * total).astype(BF16).astype(F32)
    padded = jnp.concatenate([first, first], axis=0)
    normed = normed_rows(padded, known[seqs + 1 : seqs + 2])
    for i in range(kv):
        slabs[i] = normed[:, i * span : (i + 1) * span].astype(F32)
        firsts[i] = padded[:, i * span : (i + 1) * span]
    slab = slabs[here].astype(BF16)
    first_out[...] = firsts[here][:seqs]
    xs = dot_nt(normed, w_x[...]).astype(BF16).astype(F32)
    zeta = dot_nt(normed, w_z[...]).astype(BF16).astype(F32)
    bc = dot_nn(slab, w_bc[...])
    dt = dot_nt(slab, w_dt[...])
    width = xs.shape[1]
    a = 2 * width
    b = a + bc.shape[1]
    table[:, :width] = xs
    table[:, width:a] = zeta
    table[:, a:b] = bc
    table[:, b : b + dt.shape[1]] = dt
    for d in range(kv):
        pays[d][...] = table[pl.ds(jnp.bitwise_xor(here, d), 1), :]


def state_body(kv, p0, p1, p2, p3, high, low, taps_x, past_x, taps_bc, past_bc, bias, a_log, d_skip, out, x_held, z_held, bc_held):
    here = lax.axis_index("kv")
    groups, wide = x_held.shape
    states = bc_held.shape[1]
    heads = bias.shape[1]
    pieces = (p0, p1, p2, p3)
    per = groups // kv
    width = per * wide
    for d, piece in enumerate(pieces):
        peer = jnp.bitwise_xor(here, d)
        for i in range(per):
            x_held[pl.ds(per * peer + i, 1), :] = piece[:, i * wide : (i + 1) * wide]
            z_held[pl.ds(per * peer + i, 1), :] = piece[:, width + i * wide : width + (i + 1) * wide]
    a = 2 * width
    for j in range(2 * groups):
        at = a + j * states
        bc_held[j : j + 1, :] = sum(piece[:, at : at + states] for piece in pieces)
    b = a + 2 * groups * states
    dt = sum(piece[:, b : b + heads] for piece in pieces) + bias[...]
    newest = bc_held[...].astype(BF16).astype(F32)
    steps = taps_bc.shape[0]
    mapped = newest * taps_bc[steps - 1].astype(F32)
    for k in range(steps - 1):
        mapped += past_bc[k].astype(F32) * taps_bc[k].astype(F32)
    mapped = silu(mapped)
    b_map, c_map = mapped[:groups], mapped[groups:]
    xconv = x_held[...] * taps_x[steps - 1].astype(F32)
    for k in range(steps - 1):
        xconv += past_x[k].astype(F32) * taps_x[k].astype(F32)
    xconv = silu(xconv)
    share = heads // groups
    own_group = lax.broadcasted_iota(jnp.int32, (groups, heads), 1) // share == lax.broadcasted_iota(
        jnp.int32, (groups, heads), 0
    )
    spread = (
        lax.broadcasted_iota(jnp.int32, (heads, wide), 0) % share
        == lax.broadcasted_iota(jnp.int32, (heads, wide), 1) // (wide // share)
    ).astype(F32)
    table = jnp.concatenate(
        [
            jnp.where(own_group, jnp.broadcast_to(v, (groups, heads)), 0.0)
            for v in (dt, a_log[...], d_skip[...])
        ],
        axis=0,
    )
    table = jnp.dot(table, spread, precision=lax.Precision.HIGHEST, preferred_element_type=F32)
    step = jax.nn.softplus(table[:groups])
    decay = jnp.exp(-step * jnp.exp(table[groups : 2 * groups]))
    skip = table[2 * groups :]
    c_high = c_map.astype(BF16)
    c_low = (c_map - c_high.astype(F32)).astype(BF16)
    read = dot_nt(c_high, high[...]) + dot_nt(c_low, high[...]) + dot_nt(c_high, low[...])
    read = jnp.concatenate(
        [read[g : g + 1, g * wide : (g + 1) * wide] for g in range(groups)], axis=0
    )
    inner = jnp.sum(b_map * c_map, axis=1, keepdims=True)
    mixed = (decay * read + xconv * (step * inner + skip)) * silu(z_held[...])
    mixed = mixed.astype(BF16).astype(F32)
    for g in range(groups):
        out[:, g * wide : (g + 1) * wide] = mixed[g : g + 1]


def mix_out_body(seqs, tp, m0, m1, m2, m3, w_out, first, out, table):
    here = lax.axis_index("kv")
    table[...] = jnp.zeros_like(table)
    for d, piece in enumerate((m0, m1, m2, m3)):
        table[pl.ds(jnp.bitwise_xor(here, d), 1), :] = piece[...]
    sums = dot_nn(table[...].astype(BF16), w_out[...])
    out[...] = sums[:seqs] + first[...] * (1.0 / tp)


def second_body(kv, seqs, s0, s1, s2, s3, rows, gate, up, down, *rest):
    outs, (own_out, slabs, sums_held) = rest[:kv], rest[kv:]
    here = lax.axis_index("kv")
    span = slabs.shape[2]
    for d, piece in enumerate((s0, s1, s2, s3)):
        slabs[jnp.bitwise_xor(here, d)] = piece[...].astype(F32)
    second = jnp.concatenate([slabs[i] for i in range(kv)], axis=1)
    padded = jnp.concatenate([second, second], axis=0)
    gain = rows[seqs + 2 : seqs + 3, :].astype(F32)
    sums = feed(normed_rows(padded, gain), 1, gate, up, down)[:seqs]
    for i in range(kv):
        sums_held[i] = sums[:, i * span : (i + 1) * span]
    for d in range(kv):
        outs[d][...] = sums_held[jnp.bitwise_xor(here, d)]
    own_out[...] = s0[...].astype(F32)


def small_mesh(kv, tp, *args):
    return small_step(kv, tp, *args)


def small_step(
    kv,
    tp,
    resid,
    norm_gain,
    ffn_gate,
    ffn_up,
    ffn_down,
    w_x,
    w_z,
    w_bc,
    w_dt,
    dt_bias,
    a_log,
    d_skip,
    conv_wx,
    conv_wbc,
    conv_x,
    conv_bc,
    ssm_state,
    w_out,
):
    seqs, width = resid.shape
    model = width * kv * tp
    span = model // kv
    gate, up = jnp.swapaxes(ffn_gate, 1, 2), jnp.swapaxes(ffn_up, 1, 2)
    heads = dt_bias.shape[0]
    groups, states = w_bc.shape[2:]
    half = w_x.shape[2]
    local = w_x.shape[1] * half
    wide = heads // groups * half
    flat = heads * half

    pack = run(pack_body, bf16(2 * seqs, width), (resid, norm_gain), flops=10**10)
    chip = jnp.concatenate(share_kv(pack, kv), axis=1)
    other = swap_tp(chip)
    weights = tuple(map(in_vmem, (gate, up, ffn_down)))
    sums, rows = run(
        functools.partial(first_body, kv, seqs),
        [f32(seqs, model), bf16(2 * seqs, model)],
        (chip, other, *weights),
        [pltpu.VMEM((kv * tp, 2 * seqs, width), BF16)],
    )
    sums = (sums + swap_tp(sums)).astype(BF16)
    sums = share_kv(sums, kv)

    w_xs, w_zs, w_maps, w_steps, w_join = map(
        in_vmem,
        (
            jnp.transpose(w_x, (1, 2, 0)).reshape(local, model),
            jnp.transpose(w_z, (1, 2, 0)).reshape(local, model),
            w_bc.reshape(span, 2 * groups * states),
            w_dt.T,
            w_out.reshape(flat, span),
        ),
    )
    high, low = run(
        split_body, [bf16(flat, states)] * 2, (in_vmem(ssm_state.reshape(flat, states)),)
    )
    bc_width = 2 * groups * states
    line = 2 * local + bc_width + max(heads, 128)
    *pays, first = run(
        functools.partial(mix_in_body, kv, seqs),
        [f32(1, line)] * kv + [f32(seqs, span)],
        (*sums, rows, w_xs, w_zs, w_maps, w_steps),
        [
            pltpu.VMEM((kv, 2 * seqs, span), F32),
            pltpu.VMEM((kv, 2 * seqs, span), F32),
            pltpu.VMEM((2 * seqs, line), F32),
        ],
    )
    pays = swap_kv(pays)
    mixed = run(
        functools.partial(state_body, kv),
        f32(1, flat),
        (
            *pays,
            high,
            low,
            conv_wx.reshape(-1, groups, wide),
            conv_x.reshape(-1, groups, wide),
            conv_wbc.reshape(-1, 2 * groups, states),
            conv_bc.reshape(-1, 2 * groups, states),
            dt_bias.reshape(1, heads),
            a_log.reshape(1, heads),
            d_skip.reshape(1, heads),
        ),
        [
            pltpu.VMEM((groups, wide), F32),
            pltpu.VMEM((groups, wide), F32),
            pltpu.VMEM((2 * groups, states), F32),
        ],
    )
    mixed = share_kv(mixed, kv)
    joined = run(
        functools.partial(mix_out_body, seqs, tp),
        f32(seqs, span),
        (*mixed, w_join, first),
        [pltpu.VMEM((2 * seqs, flat), F32)],
    )
    second = share_kv((joined + swap_tp(joined)).astype(BF16), kv)
    *sums, own = run(
        functools.partial(second_body, kv, seqs),
        [f32(seqs, span)] * kv + [f32(seqs, span)],
        (*second, rows, *weights),
        [pltpu.VMEM((kv, seqs, span), F32), pltpu.VMEM((kv, seqs, span), F32)],
    )
    total = sum(swap_kv(sums))
    side = lax.axis_index("tp")
    mine = lax.dynamic_slice_in_dim(total, side * width, width, 1)
    theirs = lax.dynamic_slice_in_dim(total, (1 - side) * width, width, 1)
    base = lax.dynamic_slice_in_dim(own, side * width, width, 1)
    return (base + 0.5 * (mine + swap_tp(theirs))).astype(BF16)


def normalize(rows, gain):
    values = rows.astype(jnp.float32)
    scale = lax.rsqrt(jnp.mean(values * values, axis=1, keepdims=True) + EPS)
    return (values * scale * gain.astype(jnp.float32).reshape(1, -1)).astype(jnp.bfloat16)


def feed_forward(normed, w_gate, w_up, w_down):
    gate = jnp.dot(normed, w_gate, preferred_element_type=jnp.float32)
    upper = jnp.dot(normed, w_up, preferred_element_type=jnp.float32)
    hidden = (jax.nn.silu(gate) * upper).astype(jnp.bfloat16)
    return jnp.dot(hidden, w_down, preferred_element_type=jnp.float32)


def add_half(base, sums):
    return (base.astype(jnp.float32) + 0.5 * sums).astype(jnp.bfloat16)


def ffn_totals(partial_value):
    return lax.psum(partial_value, ("kv", "tp"))


def short_conv(history, newest, taps):
    window = jnp.concatenate(
        [history.astype(jnp.float32), newest.astype(jnp.float32)[:, None]], axis=1
    )
    return jax.nn.silu(jnp.sum(window * taps.astype(jnp.float32)[None], axis=1))


def state_step(
    xs_new,
    zeta,
    bc_new,
    dt_raw,
    conv_x,
    conv_bc,
    ssm_state,
    conv_wx,
    conv_wbc,
    dt_bias,
    a_log,
    d_skip,
):
    xconv = short_conv(conv_x, xs_new, conv_wx)
    bconv = short_conv(conv_bc, bc_new, conv_wbc)
    heads = xconv.shape[1]
    groups = bconv.shape[2]
    bmat = jnp.repeat(bconv[:, 0], heads // groups, axis=1)
    cmat = jnp.repeat(bconv[:, 1], heads // groups, axis=1)
    step_size = jax.nn.softplus(dt_raw + dt_bias[None, :])
    decay = jnp.exp(-step_size * jnp.exp(a_log)[None, :])
    updated = (
        decay[:, :, None, None] * ssm_state
        + (step_size[:, :, None] * xconv)[..., None] * bmat[:, :, None, :]
    )
    mixed = (
        jnp.einsum("shpn,shn->shp", updated, cmat, precision=lax.Precision.HIGHEST)
        + d_skip[None, :, None] * xconv
    )
    return (mixed * jax.nn.silu(zeta.astype(jnp.float32))).astype(jnp.bfloat16)


def group_terms(slab, w_bc, w_dt):
    span = slab.shape[1]
    flat_bc = w_bc.reshape(span, -1)
    bc_part = jnp.dot(slab, flat_bc, preferred_element_type=jnp.float32)
    dt_part = jnp.dot(slab, w_dt, preferred_element_type=jnp.float32)
    return (
        lax.psum_scatter(bc_part, "kv", scatter_dimension=0, tiled=True),
        lax.psum_scatter(dt_part, "kv", scatter_dimension=0, tiled=True),
    )


def mix_partial(
    normed,
    w_x,
    w_z,
    w_bc,
    w_dt,
    dt_bias,
    a_log,
    d_skip,
    conv_wx,
    conv_wbc,
    conv_x,
    conv_bc,
    ssm_state,
    w_out,
):
    rows = normed.shape[0]
    local_heads = w_x.shape[1]
    half = w_x.shape[2]
    xs_part = (
        jnp.dot(normed, w_x.reshape(normed.shape[1], -1), preferred_element_type=jnp.float32)
        .astype(jnp.bfloat16)
        .reshape(rows, local_heads, half)
    )
    zeta_part = (
        jnp.dot(normed, w_z.reshape(normed.shape[1], -1), preferred_element_type=jnp.float32)
        .astype(jnp.bfloat16)
        .reshape(rows, local_heads, half)
    )
    xs_new, zeta = (
        lax.all_to_all(xs_part, "kv", split_axis=0, concat_axis=1, tiled=True),
        lax.all_to_all(zeta_part, "kv", split_axis=0, concat_axis=1, tiled=True),
    )
    span = w_bc.shape[0]
    slab = lax.dynamic_slice_in_dim(normed, lax.axis_index("kv") * span, span, 1)
    bc_sum, dt_raw = group_terms(slab, w_bc, w_dt)
    bc_new = bc_sum.astype(jnp.bfloat16).reshape((bc_sum.shape[0],) + w_bc.shape[1:])
    mixed = state_step(
        xs_new,
        zeta,
        bc_new,
        dt_raw,
        conv_x,
        conv_bc,
        ssm_state,
        conv_wx,
        conv_wbc,
        dt_bias,
        a_log,
        d_skip,
    )
    flat_out = w_out.reshape(-1, w_out.shape[2])
    piece = lax.all_gather(mixed, "kv", axis=0, tiled=True)
    return jnp.dot(piece.reshape(piece.shape[0], -1), flat_out, preferred_element_type=jnp.float32)


def per_device(
    resid,
    norm_gain,
    ffn_gate,
    ffn_up,
    ffn_down,
    w_x,
    w_z,
    w_bc,
    w_dt,
    dt_bias,
    a_log,
    d_skip,
    conv_wx,
    conv_wbc,
    conv_x,
    conv_bc,
    ssm_state,
    w_out,
):
    mixer_args = (
        w_x,
        w_z,
        w_bc,
        w_dt,
        dt_bias,
        a_log,
        d_skip,
        conv_wx,
        conv_wbc,
        conv_x,
        conv_bc,
        ssm_state,
        w_out,
    )
    rows, gains = (
        lax.all_gather(resid, ("kv", "tp"), axis=1, tiled=True),
        lax.all_gather(norm_gain, ("kv", "tp"), axis=1, tiled=True),
    )
    first = add_half(
        rows,
        ffn_totals(feed_forward(normalize(rows, gains[0]), ffn_gate[0], ffn_up[0], ffn_down[0])),
    )
    partial_value = mix_partial(normalize(first, gains[1]), *mixer_args)
    span = partial_value.shape[1]
    block = lax.dynamic_slice_in_dim(first, lax.axis_index("kv") * span, span, 1)
    joined = (block.astype(jnp.float32) + lax.psum(partial_value, "tp")).astype(jnp.bfloat16)
    second = lax.all_gather(joined, "kv", axis=1, tiled=True)
    final = add_half(
        second,
        ffn_totals(feed_forward(normalize(second, gains[2]), ffn_gate[1], ffn_up[1], ffn_down[1])),
    )
    width = resid.shape[1]
    return lax.dynamic_slice_in_dim(final, lax.axis_index(("kv", "tp")) * width, width, 1)


def solution(mesh):
    placed = (
        P("dp", ("kv", "tp")),
        P(None, ("kv", "tp")),
        P(None, None, ("kv", "tp")),
        P(None, None, ("kv", "tp")),
        P(None, ("kv", "tp"), None),
        P(None, "kv", "tp"),
        P(None, "kv", "tp"),
        P("kv", None, None, None),
        P("kv", None),
        P(),
        P(),
        P(),
        P(None, None, "tp"),
        P(),
        P(("dp", "kv"), None, None, "tp"),
        P(("dp", "kv"), None, None, None, None),
        P(("dp", "kv"), None, "tp", None),
        P(None, "tp", "kv"),
    )
    kv, tp = mesh.shape["kv"], mesh.shape["tp"]
    small = (kv, tp) == (4, 2)
    return jax.shard_map(
        functools.partial(small_mesh, kv, tp) if small else per_device,
        mesh=mesh,
        in_specs=placed,
        out_specs=P("dp", ("kv", "tp")),
        check_vma=False,
    )
```

```python
import functools

import jax
import jax.numpy as jnp
from jax import lax
from jax.experimental import pallas as pl
from jax.experimental.pallas import tpu as pltpu
from jax.sharding import PartitionSpec as P


EPS = 1e-06
F32 = jnp.float32
BF16 = jnp.bfloat16
NT = (((1,), (1,)), ((), ()))
HBM = pl.BlockSpec(memory_space=pltpu.HBM)
VMEM = pl.BlockSpec(memory_space=pltpu.VMEM)


def dot_nt(left, right):
    return lax.dot_general(left, right, NT, preferred_element_type=F32)


def dot_nn(left, right):
    return jnp.dot(left, right, preferred_element_type=F32)


def silu(value):
    return value * jax.nn.sigmoid(value)


def swap_kv(values):
    kv = len(values)
    got = list(values)
    for d in reversed(range(1, kv)):
        got[d] = lax.ppermute(values[d], "kv", [(i, i ^ d) for i in range(kv)])
    return got


def share_kv(value, kv):
    return swap_kv([value] * kv)


def swap_tp(value):
    return lax.ppermute(value, "tp", [(0, 1), (1, 0)])


def in_vmem(value):
    return pltpu.with_memory_space_constraint(value, pltpu.VMEM)


def in_hbm(value):
    return pltpu.with_memory_space_constraint(value, pltpu.HBM)


def run(body, outs, args, scratch=(), limit=16, in_specs=None, flops=10**10):
    return pl.pallas_call(
        body,
        out_shape=outs,
        in_specs=in_specs or [VMEM] * len(args),
        out_specs=jax.tree.map(lambda _: VMEM, outs),
        scratch_shapes=list(scratch),
        compiler_params=pltpu.CompilerParams(vmem_limit_bytes=limit * 2**20),
        cost_estimate=pl.CostEstimate(flops=flops, bytes_accessed=0, transcendentals=0),
    )(*args)


def f32(*shape):
    return jax.ShapeDtypeStruct(shape, F32)


def bf16(*shape):
    return jax.ShapeDtypeStruct(shape, BF16)


def split_body(state, high_out, low_out):
    values = state[...]
    high = values.astype(BF16)
    high_out[...] = high
    low_out[...] = (values - high.astype(F32)).astype(BF16)


def normed_rows(values, gain):
    scale = lax.rsqrt(jnp.mean(values * values, axis=1, keepdims=True) + EPS)
    return (values * scale * gain).astype(BF16)


def feed(normed, layer, gate, up, down):
    if len(gate.shape) == 3:
        gated, upper = dot_nt(normed, gate[layer]), dot_nt(normed, up[layer])
    else:
        gated, upper = dot_nn(normed, gate[...]), dot_nn(normed, up[...])
    return dot_nn((silu(gated) * upper).astype(BF16), down[layer])


def pack_body(rows, gains, out, rows_held, gains_held, sems):
    copies = (
        pltpu.make_async_copy(rows, rows_held, sems.at[0]),
        pltpu.make_async_copy(gains, gains_held, sems.at[1]),
    )
    for copy in copies:
        copy.start()
    for copy in copies:
        copy.wait()
    seqs, count = rows_held.shape[0], gains_held.shape[0]
    out[:seqs] = rows_held[...]
    out[seqs : seqs + count] = gains_held[...]
    out[seqs + count :] = gains_held[:1]


def turn_body(*refs):
    count = len(refs) // 2
    for source, target in zip(refs[:count], refs[count:]):
        target[...] = source[...].T


def turned(sources):
    outs = run(
        turn_body, [bf16(*source.shape[::-1]) for source in sources], tuple(map(in_vmem, sources))
    )
    return [in_vmem(out) for out in outs]


TURN = 256


def turn_layer_body(layer, source, target, held, sems):
    height = held.shape[0]
    blocks = [pl.ds(i, min(TURN, height - i)) for i in range(0, height, TURN)]
    copies = [
        pltpu.make_async_copy(source.at[layer, rows], held.at[rows], sems.at[i])
        for i, rows in enumerate(blocks)
    ]
    for copy in copies:
        copy.start()
    for copy, rows in zip(copies, blocks):
        copy.wait()
        target[:, rows] = held[rows].T


def turned_layer(source, layer):
    height, wide = source.shape[1:]
    out = run(
        functools.partial(turn_layer_body, layer),
        bf16(wide, height),
        (in_hbm(source),),
        [
            pltpu.VMEM((height, wide), BF16),
            pltpu.SemaphoreType.DMA((pl.cdiv(height, TURN),)),
        ],
        in_specs=[HBM],
    )
    return in_vmem(out)


def first_body(kv, seqs, own, other, gate, up, down, sums_out, rows_out, slabs):
    here, side = lax.axis_index("kv"), lax.axis_index("tp")
    width = slabs.shape[2]
    for d in range(kv):
        peer = jnp.bitwise_xor(here, d)
        slabs[2 * peer + side] = own[:, d * width : (d + 1) * width]
        slabs[2 * peer + 1 - side] = other[:, d * width : (d + 1) * width]
    rows = jnp.concatenate([slabs[i] for i in range(slabs.shape[0])], axis=1)
    rows_out[...] = rows
    values = rows.astype(F32)
    sums = feed(normed_rows(values, values[seqs : seqs + 1]), 0, gate, up, down)
    sums_out[...] = sums[:seqs]


def mix_in_body(kv, seqs, s0, s1, s2, s3, rows, w_x, w_z, w_bc, w_dt, *rest):
    pays, (first_out, slabs, firsts, table) = rest[:kv], rest[kv:]
    here = lax.axis_index("kv")
    span = slabs.shape[2]
    total = s0[...].astype(F32) + s1[...].astype(F32) + s2[...].astype(F32) + s3[...].astype(F32)
    known = rows[...].astype(F32)
    first = (known[:seqs] + 0.5 * total).astype(BF16).astype(F32)
    padded = jnp.concatenate([first, first], axis=0)
    normed = normed_rows(padded, known[seqs + 1 : seqs + 2])
    for i in range(kv):
        slabs[i] = normed[:, i * span : (i + 1) * span].astype(F32)
        firsts[i] = padded[:, i * span : (i + 1) * span]
    slab = slabs[here].astype(BF16)
    first_out[...] = firsts[here][:seqs]
    xs = dot_nn(normed, w_x[...]).astype(BF16).astype(F32)
    zeta = dot_nn(normed, w_z[...]).astype(BF16).astype(F32)
    bc = dot_nn(slab, w_bc[...])
    dt = dot_nt(slab, w_dt[...])
    width = xs.shape[1]
    a = 2 * width
    b = a + bc.shape[1]
    table[:, :width] = xs
    table[:, width:a] = zeta
    table[:, a:b] = bc
    table[:, b : b + dt.shape[1]] = dt
    for d in range(kv):
        pays[d][...] = table[pl.ds(jnp.bitwise_xor(here, d), 1), :]


def state_body(kv, p0, p1, p2, p3, high, low, taps_x, past_x, taps_bc, past_bc, bias, a_log, d_skip, out, x_held, z_held, bc_held):
    here = lax.axis_index("kv")
    groups, wide = x_held.shape
    states = bc_held.shape[1]
    heads = bias.shape[1]
    pieces = (p0, p1, p2, p3)
    per = groups // kv
    width = per * wide
    for d, piece in enumerate(pieces):
        peer = jnp.bitwise_xor(here, d)
        for i in range(per):
            x_held[pl.ds(per * peer + i, 1), :] = piece[:, i * wide : (i + 1) * wide]
            z_held[pl.ds(per * peer + i, 1), :] = piece[:, width + i * wide : width + (i + 1) * wide]
    a = 2 * width
    for j in range(2 * groups):
        at = a + j * states
        bc_held[j : j + 1, :] = sum(piece[:, at : at + states] for piece in pieces)
    b = a + 2 * groups * states
    dt = sum(piece[:, b : b + heads] for piece in pieces) + bias[...]
    newest = bc_held[...].astype(BF16).astype(F32)
    steps = taps_bc.shape[0]
    mapped = newest * taps_bc[steps - 1].astype(F32)
    for k in range(steps - 1):
        mapped += past_bc[k].astype(F32) * taps_bc[k].astype(F32)
    mapped = silu(mapped)
    b_map, c_map = mapped[:groups], mapped[groups:]
    xconv = x_held[...] * taps_x[steps - 1].astype(F32)
    for k in range(steps - 1):
        xconv += past_x[k].astype(F32) * taps_x[k].astype(F32)
    xconv = silu(xconv)
    share = heads // groups
    own_group = lax.broadcasted_iota(jnp.int32, (groups, heads), 1) // share == lax.broadcasted_iota(
        jnp.int32, (groups, heads), 0
    )
    spread = (
        lax.broadcasted_iota(jnp.int32, (heads, wide), 0) % share
        == lax.broadcasted_iota(jnp.int32, (heads, wide), 1) // (wide // share)
    ).astype(F32)
    table = jnp.concatenate(
        [
            jnp.where(own_group, jnp.broadcast_to(v, (groups, heads)), 0.0)
            for v in (dt, a_log[...], d_skip[...])
        ],
        axis=0,
    )
    table = jnp.dot(table, spread, precision=lax.Precision.HIGHEST, preferred_element_type=F32)
    step = jax.nn.softplus(table[:groups])
    decay = jnp.exp(-step * jnp.exp(table[groups : 2 * groups]))
    skip = table[2 * groups :]
    c_high = c_map.astype(BF16)
    c_low = (c_map - c_high.astype(F32)).astype(BF16)
    read = dot_nt(c_high, high[...]) + dot_nt(c_low, high[...]) + dot_nt(c_high, low[...])
    read = jnp.concatenate(
        [read[g : g + 1, g * wide : (g + 1) * wide] for g in range(groups)], axis=0
    )
    inner = jnp.sum(b_map * c_map, axis=1, keepdims=True)
    mixed = (decay * read + xconv * (step * inner + skip)) * silu(z_held[...])
    mixed = mixed.astype(BF16).astype(F32)
    for g in range(groups):
        out[:, g * wide : (g + 1) * wide] = mixed[g : g + 1]


def mix_out_body(seqs, tp, m0, m1, m2, m3, w_out, first, out, table):
    here = lax.axis_index("kv")
    table[...] = jnp.zeros_like(table)
    for d, piece in enumerate((m0, m1, m2, m3)):
        table[pl.ds(jnp.bitwise_xor(here, d), 1), :] = piece[...]
    sums = dot_nn(table[...].astype(BF16), w_out[...])
    out[...] = sums[:seqs] + first[...] * (1.0 / tp)


def second_body(kv, seqs, s0, s1, s2, s3, rows, gate, up, down, *rest):
    outs, (own_out, slabs, sums_held) = rest[:kv], rest[kv:]
    here = lax.axis_index("kv")
    span = slabs.shape[2]
    for d, piece in enumerate((s0, s1, s2, s3)):
        slabs[jnp.bitwise_xor(here, d)] = piece[...].astype(F32)
    second = jnp.concatenate([slabs[i] for i in range(kv)], axis=1)
    padded = jnp.concatenate([second, second], axis=0)
    gain = rows[seqs + 2 : seqs + 3, :].astype(F32)
    sums = feed(normed_rows(padded, gain), 1, gate, up, down)[:seqs]
    for i in range(kv):
        sums_held[i] = sums[:, i * span : (i + 1) * span]
    for d in range(kv):
        outs[d][...] = sums_held[jnp.bitwise_xor(here, d)]
    own_out[...] = s0[...].astype(F32)


def small_mesh(kv, tp, *args):
    return small_step(kv, tp, *args)


def small_step(
    kv,
    tp,
    resid,
    norm_gain,
    ffn_gate,
    ffn_up,
    ffn_down,
    w_x,
    w_z,
    w_bc,
    w_dt,
    dt_bias,
    a_log,
    d_skip,
    conv_wx,
    conv_wbc,
    conv_x,
    conv_bc,
    ssm_state,
    w_out,
):
    seqs, width = resid.shape
    model = width * kv * tp
    span = model // kv
    gate, up = jnp.swapaxes(ffn_gate, 1, 2), jnp.swapaxes(ffn_up, 1, 2)
    heads = dt_bias.shape[0]
    groups, states = w_bc.shape[2:]
    half = w_x.shape[2]
    local = w_x.shape[1] * half
    wide = heads // groups * half
    flat = heads * half

    pack = run(
        pack_body,
        bf16(2 * seqs, width),
        (in_hbm(resid), in_hbm(norm_gain)),
        [
            pltpu.VMEM(resid.shape, BF16),
            pltpu.VMEM(norm_gain.shape, BF16),
            pltpu.SemaphoreType.DMA((2,)),
        ],
        in_specs=[HBM] * 2,
    )
    chip = jnp.concatenate(share_kv(pack, kv), axis=1)
    other = swap_tp(chip)
    down = in_vmem(ffn_down)

    sums, rows = run(
        functools.partial(first_body, kv, seqs),
        [f32(seqs, model), bf16(2 * seqs, model)],
        (chip, other, in_vmem(gate), in_vmem(up), down),
        [pltpu.VMEM((kv * tp, 2 * seqs, width), BF16)],
    )
    sums = (sums + swap_tp(sums)).astype(BF16)
    sums = share_kv(sums, kv)

    w_xs, w_zs = turned([jnp.transpose(w, (1, 2, 0)).reshape(local, model) for w in (w_x, w_z)])
    w_maps, w_steps, w_join = map(
        in_vmem,
        (
            w_bc.reshape(span, 2 * groups * states),
            w_dt.T,
            w_out.reshape(flat, span),
        ),
    )
    high, low = run(
        split_body, [bf16(flat, states)] * 2, (in_vmem(ssm_state.reshape(flat, states)),)
    )
    bc_width = 2 * groups * states
    line = 2 * local + bc_width + max(heads, 128)
    *pays, first = run(
        functools.partial(mix_in_body, kv, seqs),
        [f32(1, line)] * kv + [f32(seqs, span)],
        (*sums, rows, w_xs, w_zs, w_maps, w_steps),
        [
            pltpu.VMEM((kv, 2 * seqs, span), F32),
            pltpu.VMEM((kv, 2 * seqs, span), F32),
            pltpu.VMEM((2 * seqs, line), F32),
        ],
    )
    pays = swap_kv(pays)
    mixed = run(
        functools.partial(state_body, kv),
        f32(1, flat),
        (
            *pays,
            high,
            low,
            conv_wx.reshape(-1, groups, wide),
            conv_x.reshape(-1, groups, wide),
            conv_wbc.reshape(-1, 2 * groups, states),
            conv_bc.reshape(-1, 2 * groups, states),
            dt_bias.reshape(1, heads),
            a_log.reshape(1, heads),
            d_skip.reshape(1, heads),
        ),
        [
            pltpu.VMEM((groups, wide), F32),
            pltpu.VMEM((groups, wide), F32),
            pltpu.VMEM((2 * groups, states), F32),
        ],
    )
    mixed = share_kv(mixed, kv)
    joined = run(
        functools.partial(mix_out_body, seqs, tp),
        f32(seqs, span),
        (*mixed, w_join, first),
        [pltpu.VMEM((2 * seqs, flat), F32)],
    )
    second = share_kv((joined + swap_tp(joined)).astype(BF16), kv)
    gate_two = turned_layer(gate, 1)
    up_two = turned_layer(up, 1)
    *sums, own = run(
        functools.partial(second_body, kv, seqs),
        [f32(seqs, span)] * kv + [f32(seqs, span)],
        (*second, rows, gate_two, up_two, down),
        [pltpu.VMEM((kv, seqs, span), F32), pltpu.VMEM((kv, seqs, span), F32)],
    )
    total = sum(swap_kv(sums))
    side = lax.axis_index("tp")
    mine = lax.dynamic_slice_in_dim(total, side * width, width, 1)
    theirs = lax.dynamic_slice_in_dim(total, (1 - side) * width, width, 1)
    base = lax.dynamic_slice_in_dim(own, side * width, width, 1)
    return (base + 0.5 * (mine + swap_tp(theirs))).astype(BF16)


def normalize(rows, gain):
    values = rows.astype(jnp.float32)
    scale = lax.rsqrt(jnp.mean(values * values, axis=1, keepdims=True) + EPS)
    return (values * scale * gain.astype(jnp.float32).reshape(1, -1)).astype(jnp.bfloat16)


def feed_forward(normed, w_gate, w_up, w_down):
    gate = jnp.dot(normed, w_gate, preferred_element_type=jnp.float32)
    upper = jnp.dot(normed, w_up, preferred_element_type=jnp.float32)
    hidden = (jax.nn.silu(gate) * upper).astype(jnp.bfloat16)
    return jnp.dot(hidden, w_down, preferred_element_type=jnp.float32)


def add_half(base, sums):
    return (base.astype(jnp.float32) + 0.5 * sums).astype(jnp.bfloat16)


def ffn_totals(partial_value):
    return lax.psum(partial_value, ("kv", "tp"))


def short_conv(history, newest, taps):
    window = jnp.concatenate(
        [history.astype(jnp.float32), newest.astype(jnp.float32)[:, None]], axis=1
    )
    return jax.nn.silu(jnp.sum(window * taps.astype(jnp.float32)[None], axis=1))


def state_step(
    xs_new,
    zeta,
    bc_new,
    dt_raw,
    conv_x,
    conv_bc,
    ssm_state,
    conv_wx,
    conv_wbc,
    dt_bias,
    a_log,
    d_skip,
):
    xconv = short_conv(conv_x, xs_new, conv_wx)
    bconv = short_conv(conv_bc, bc_new, conv_wbc)
    heads = xconv.shape[1]
    groups = bconv.shape[2]
    bmat = jnp.repeat(bconv[:, 0], heads // groups, axis=1)
    cmat = jnp.repeat(bconv[:, 1], heads // groups, axis=1)
    step_size = jax.nn.softplus(dt_raw + dt_bias[None, :])
    decay = jnp.exp(-step_size * jnp.exp(a_log)[None, :])
    updated = (
        decay[:, :, None, None] * ssm_state
        + (step_size[:, :, None] * xconv)[..., None] * bmat[:, :, None, :]
    )
    mixed = (
        jnp.einsum("shpn,shn->shp", updated, cmat, precision=lax.Precision.HIGHEST)
        + d_skip[None, :, None] * xconv
    )
    return (mixed * jax.nn.silu(zeta.astype(jnp.float32))).astype(jnp.bfloat16)


def group_terms(slab, w_bc, w_dt):
    span = slab.shape[1]
    flat_bc = w_bc.reshape(span, -1)
    bc_part = jnp.dot(slab, flat_bc, preferred_element_type=jnp.float32)
    dt_part = jnp.dot(slab, w_dt, preferred_element_type=jnp.float32)
    return (
        lax.psum_scatter(bc_part, "kv", scatter_dimension=0, tiled=True),
        lax.psum_scatter(dt_part, "kv", scatter_dimension=0, tiled=True),
    )


def mix_partial(
    normed,
    w_x,
    w_z,
    w_bc,
    w_dt,
    dt_bias,
    a_log,
    d_skip,
    conv_wx,
    conv_wbc,
    conv_x,
    conv_bc,
    ssm_state,
    w_out,
):
    rows = normed.shape[0]
    local_heads = w_x.shape[1]
    half = w_x.shape[2]
    xs_part = (
        jnp.dot(normed, w_x.reshape(normed.shape[1], -1), preferred_element_type=jnp.float32)
        .astype(jnp.bfloat16)
        .reshape(rows, local_heads, half)
    )
    zeta_part = (
        jnp.dot(normed, w_z.reshape(normed.shape[1], -1), preferred_element_type=jnp.float32)
        .astype(jnp.bfloat16)
        .reshape(rows, local_heads, half)
    )
    xs_new, zeta = (
        lax.all_to_all(xs_part, "kv", split_axis=0, concat_axis=1, tiled=True),
        lax.all_to_all(zeta_part, "kv", split_axis=0, concat_axis=1, tiled=True),
    )
    span = w_bc.shape[0]
    slab = lax.dynamic_slice_in_dim(normed, lax.axis_index("kv") * span, span, 1)
    bc_sum, dt_raw = group_terms(slab, w_bc, w_dt)
    bc_new = bc_sum.astype(jnp.bfloat16).reshape((bc_sum.shape[0],) + w_bc.shape[1:])
    mixed = state_step(
        xs_new,
        zeta,
        bc_new,
        dt_raw,
        conv_x,
        conv_bc,
        ssm_state,
        conv_wx,
        conv_wbc,
        dt_bias,
        a_log,
        d_skip,
    )
    flat_out = w_out.reshape(-1, w_out.shape[2])
    piece = lax.all_gather(mixed, "kv", axis=0, tiled=True)
    return jnp.dot(piece.reshape(piece.shape[0], -1), flat_out, preferred_element_type=jnp.float32)


def per_device(
    resid,
    norm_gain,
    ffn_gate,
    ffn_up,
    ffn_down,
    w_x,
    w_z,
    w_bc,
    w_dt,
    dt_bias,
    a_log,
    d_skip,
    conv_wx,
    conv_wbc,
    conv_x,
    conv_bc,
    ssm_state,
    w_out,
):
    mixer_args = (
        w_x,
        w_z,
        w_bc,
        w_dt,
        dt_bias,
        a_log,
        d_skip,
        conv_wx,
        conv_wbc,
        conv_x,
        conv_bc,
        ssm_state,
        w_out,
    )
    rows, gains = (
        lax.all_gather(resid, ("kv", "tp"), axis=1, tiled=True),
        lax.all_gather(norm_gain, ("kv", "tp"), axis=1, tiled=True),
    )
    first = add_half(
        rows,
        ffn_totals(feed_forward(normalize(rows, gains[0]), ffn_gate[0], ffn_up[0], ffn_down[0])),
    )
    partial_value = mix_partial(normalize(first, gains[1]), *mixer_args)
    span = partial_value.shape[1]
    block = lax.dynamic_slice_in_dim(first, lax.axis_index("kv") * span, span, 1)
    joined = (block.astype(jnp.float32) + lax.psum(partial_value, "tp")).astype(jnp.bfloat16)
    second = lax.all_gather(joined, "kv", axis=1, tiled=True)
    final = add_half(
        second,
        ffn_totals(feed_forward(normalize(second, gains[2]), ffn_gate[1], ffn_up[1], ffn_down[1])),
    )
    width = resid.shape[1]
    return lax.dynamic_slice_in_dim(final, lax.axis_index(("kv", "tp")) * width, width, 1)


def solution(mesh):
    placed = (
        P("dp", ("kv", "tp")),
        P(None, ("kv", "tp")),
        P(None, None, ("kv", "tp")),
        P(None, None, ("kv", "tp")),
        P(None, ("kv", "tp"), None),
        P(None, "kv", "tp"),
        P(None, "kv", "tp"),
        P("kv", None, None, None),
        P("kv", None),
        P(),
        P(),
        P(),
        P(None, None, "tp"),
        P(),
        P(("dp", "kv"), None, None, "tp"),
        P(("dp", "kv"), None, None, None, None),
        P(("dp", "kv"), None, "tp", None),
        P(None, "tp", "kv"),
    )
    kv, tp = mesh.shape["kv"], mesh.shape["tp"]
    small = (kv, tp) == (4, 2)
    return jax.shard_map(
        functools.partial(small_mesh, kv, tp) if small else per_device,
        mesh=mesh,
        in_specs=placed,
        out_specs=P("dp", ("kv", "tp")),
        check_vma=False,
    )
```

```python
import functools

import jax
import jax.numpy as jnp
from jax import lax
from jax.experimental import pallas as pl
from jax.experimental.pallas import tpu as pltpu
from jax.sharding import PartitionSpec as P


EPS = 1e-06
F32 = jnp.float32
BF16 = jnp.bfloat16
NT = (((1,), (1,)), ((), ()))
HBM = pl.BlockSpec(memory_space=pltpu.HBM)
VMEM = pl.BlockSpec(memory_space=pltpu.VMEM)


def dot_nt(left, right):
    return lax.dot_general(left, right, NT, preferred_element_type=F32)


def dot_nn(left, right):
    return jnp.dot(left, right, preferred_element_type=F32)


def silu(value):
    return value * jax.nn.sigmoid(value)


def swap_kv(values):
    kv = len(values)
    got = list(values)
    for d in reversed(range(1, kv)):
        got[d] = lax.ppermute(values[d], "kv", [(i, i ^ d) for i in range(kv)])
    return got


def share_kv(value, kv):
    return swap_kv([value] * kv)


def swap_tp(value):
    return lax.ppermute(value, "tp", [(0, 1), (1, 0)])


def swap_far(value):
    pairs = [(2 * c + t, 2 * (c ^ (2 + t)) + t) for c in range(4) for t in range(2)]
    return lax.ppermute(value, ("kv", "tp"), pairs)


def swap_near(value):
    pairs = [(2 * c + t, 2 * (c ^ 1) + t) for c in range(4) for t in range(2)]
    return lax.ppermute(value, ("kv", "tp"), pairs)


def share_chip(value):
    far = swap_far(value)
    near = swap_near(value)
    return [value, near, far, swap_tp(far)]


def peers(here, side):
    return [jnp.bitwise_xor(here, d) for d in (0, 1, 2 + side, 3 - side)]


def in_vmem(value):
    return pltpu.with_memory_space_constraint(value, pltpu.VMEM)


def in_hbm(value):
    return pltpu.with_memory_space_constraint(value, pltpu.HBM)


def run(body, outs, args, scratch=(), limit=16, in_specs=None, flops=10**10):
    return pl.pallas_call(
        body,
        out_shape=outs,
        in_specs=in_specs or [VMEM] * len(args),
        out_specs=jax.tree.map(lambda _: VMEM, outs),
        scratch_shapes=list(scratch),
        compiler_params=pltpu.CompilerParams(vmem_limit_bytes=limit * 2**20),
        cost_estimate=pl.CostEstimate(flops=flops, bytes_accessed=0, transcendentals=0),
    )(*args)


def f32(*shape):
    return jax.ShapeDtypeStruct(shape, F32)


def bf16(*shape):
    return jax.ShapeDtypeStruct(shape, BF16)


def split_body(state, high_out, low_out):
    values = state[...]
    high = values.astype(BF16)
    high_out[...] = high
    low_out[...] = (values - high.astype(F32)).astype(BF16)


def normed_rows(values, gain):
    scale = lax.rsqrt(jnp.mean(values * values, axis=1, keepdims=True) + EPS)
    return (values * scale * gain).astype(BF16)


def project(normed, layer, weights):
    if len(weights.shape) == 3:
        return dot_nt(normed, weights[layer])
    return dot_nn(normed, weights[...])


def feed(normed, layer, gate, up, down):
    gated, upper = project(normed, layer, gate), project(normed, layer, up)
    return dot_nn((silu(gated) * upper).astype(BF16), down[layer])


def pack_body(rows, gains, out, rows_held, gains_held, sems):
    copies = (
        pltpu.make_async_copy(rows, rows_held, sems.at[0]),
        pltpu.make_async_copy(gains, gains_held, sems.at[1]),
    )
    for copy in copies:
        copy.start()
    for copy in copies:
        copy.wait()
    seqs, count = rows_held.shape[0], gains_held.shape[0]
    out[:seqs] = rows_held[...]
    out[seqs : seqs + count] = gains_held[...]
    out[seqs + count :] = gains_held[:1]


def turn_body(*refs):
    count = len(refs) // 2
    for source, target in zip(refs[:count], refs[count:]):
        target[...] = source[...].T


def turned(sources):
    outs = run(
        turn_body, [bf16(*source.shape[::-1]) for source in sources], tuple(map(in_vmem, sources))
    )
    return [in_vmem(out) for out in outs]


TURN = 256


def turn_layer_body(layer, source, target, held, sems):
    height = held.shape[0]
    blocks = [pl.ds(i, min(TURN, height - i)) for i in range(0, height, TURN)]
    copies = [
        pltpu.make_async_copy(source.at[layer, rows], held.at[rows], sems.at[i])
        for i, rows in enumerate(blocks)
    ]
    for copy in copies:
        copy.start()
    for copy, rows in zip(copies, blocks):
        copy.wait()
        target[:, rows] = held[rows].T


def turn_held_body(layer, source, target):
    target[...] = source[layer].T


def turned_held(source, layer):
    out = run(
        functools.partial(turn_held_body, layer), bf16(*source.shape[:0:-1]), (in_vmem(source),)
    )
    return in_vmem(out)


def turned_layer(source, layer):
    height, wide = source.shape[1:]
    out = run(
        functools.partial(turn_layer_body, layer),
        bf16(wide, height),
        (in_hbm(source),),
        [
            pltpu.VMEM((height, wide), BF16),
            pltpu.SemaphoreType.DMA((pl.cdiv(height, TURN),)),
        ],
        in_specs=[HBM],
    )
    return in_vmem(out)


def first_body(seqs, c0, c1, c2, c3, gate, up, down, sums_out, rows_out, slabs):
    here, side = lax.axis_index("kv"), lax.axis_index("tp")
    width = slabs.shape[2]
    for peer, piece, first in zip(peers(here, side), (c0, c1, c2, c3), (side, side, side, 1 - side)):
        slabs[2 * peer + first] = piece[:, :width]
        slabs[2 * peer + 1 - first] = piece[:, width:]
    rows = jnp.concatenate([slabs[i] for i in range(slabs.shape[0])], axis=1)
    rows_out[...] = rows
    values = rows.astype(F32)
    sums = feed(normed_rows(values, values[seqs : seqs + 1]), 0, gate, up, down)
    sums_out[...] = sums[:seqs]


def mix_in_body(kv, seqs, s0, s1, s2, s3, rows, w_x, w_z, w_bc, w_dt, *rest):
    pays, (first_out, slabs, firsts, table) = rest[:kv], rest[kv:]
    here = lax.axis_index("kv")
    span = slabs.shape[2]
    total = s0[...].astype(F32) + s1[...].astype(F32) + s2[...].astype(F32) + s3[...].astype(F32)
    known = rows[...].astype(F32)
    first = (known[:seqs] + 0.5 * total).astype(BF16).astype(F32)
    padded = jnp.concatenate([first, first], axis=0)
    normed = normed_rows(padded, known[seqs + 1 : seqs + 2])
    for i in range(kv):
        slabs[i] = normed[:, i * span : (i + 1) * span].astype(F32)
        firsts[i] = padded[:, i * span : (i + 1) * span]
    slab = slabs[here].astype(BF16)
    first_out[...] = firsts[here][:seqs]
    xs = dot_nn(normed, w_x[...]).astype(BF16).astype(F32)
    zeta = dot_nn(normed, w_z[...]).astype(BF16).astype(F32)
    bc = dot_nn(slab, w_bc[...])
    dt = dot_nt(slab, w_dt[...])
    width = xs.shape[1]
    a = 2 * width
    b = a + bc.shape[1]
    table[:, :width] = xs
    table[:, width:a] = zeta
    table[:, a:b] = bc
    table[:, b : b + dt.shape[1]] = dt
    for d in range(kv):
        pays[d][...] = table[pl.ds(jnp.bitwise_xor(here, d), 1), :]


def state_body(kv, p0, p1, p2, p3, high, low, taps_x, past_x, taps_bc, past_bc, bias, a_log, d_skip, out, x_held, z_held, bc_held):
    here = lax.axis_index("kv")
    groups, wide = x_held.shape
    states = bc_held.shape[1]
    heads = bias.shape[1]
    pieces = (p0, p1, p2, p3)
    per = groups // kv
    width = per * wide
    for d, piece in enumerate(pieces):
        peer = jnp.bitwise_xor(here, d)
        for i in range(per):
            x_held[pl.ds(per * peer + i, 1), :] = piece[:, i * wide : (i + 1) * wide]
            z_held[pl.ds(per * peer + i, 1), :] = piece[:, width + i * wide : width + (i + 1) * wide]
    a = 2 * width
    for j in range(2 * groups):
        at = a + j * states
        bc_held[j : j + 1, :] = sum(piece[:, at : at + states] for piece in pieces)
    b = a + 2 * groups * states
    dt = sum(piece[:, b : b + heads] for piece in pieces) + bias[...]
    newest = bc_held[...].astype(BF16).astype(F32)
    steps = taps_bc.shape[0]
    mapped = newest * taps_bc[steps - 1].astype(F32)
    for k in range(steps - 1):
        mapped += past_bc[k].astype(F32) * taps_bc[k].astype(F32)
    mapped = silu(mapped)
    b_map, c_map = mapped[:groups], mapped[groups:]
    xconv = x_held[...] * taps_x[steps - 1].astype(F32)
    for k in range(steps - 1):
        xconv += past_x[k].astype(F32) * taps_x[k].astype(F32)
    xconv = silu(xconv)
    share = heads // groups
    own_group = lax.broadcasted_iota(jnp.int32, (groups, heads), 1) // share == lax.broadcasted_iota(
        jnp.int32, (groups, heads), 0
    )
    spread = (
        lax.broadcasted_iota(jnp.int32, (heads, wide), 0) % share
        == lax.broadcasted_iota(jnp.int32, (heads, wide), 1) // (wide // share)
    ).astype(F32)
    table = jnp.concatenate(
        [
            jnp.where(own_group, jnp.broadcast_to(v, (groups, heads)), 0.0)
            for v in (dt, a_log[...], d_skip[...])
        ],
        axis=0,
    )
    table = jnp.dot(table, spread, precision=lax.Precision.HIGHEST, preferred_element_type=F32)
    step = jax.nn.softplus(table[:groups])
    decay = jnp.exp(-step * jnp.exp(table[groups : 2 * groups]))
    skip = table[2 * groups :]
    c_high = c_map.astype(BF16)
    c_low = (c_map - c_high.astype(F32)).astype(BF16)
    read = dot_nt(c_high, high[...]) + dot_nt(c_low, high[...]) + dot_nt(c_high, low[...])
    read = jnp.concatenate(
        [read[g : g + 1, g * wide : (g + 1) * wide] for g in range(groups)], axis=0
    )
    inner = jnp.sum(b_map * c_map, axis=1, keepdims=True)
    mixed = (decay * read + xconv * (step * inner + skip)) * silu(z_held[...])
    mixed = mixed.astype(BF16).astype(F32)
    for g in range(groups):
        out[:, g * wide : (g + 1) * wide] = mixed[g : g + 1]


def mix_out_body(seqs, tp, m0, m1, m2, m3, w_out, first, out, table):
    here = lax.axis_index("kv")
    table[...] = jnp.zeros_like(table)
    for d, piece in enumerate((m0, m1, m2, m3)):
        table[pl.ds(jnp.bitwise_xor(here, d), 1), :] = piece[...]
    sums = dot_nn(table[...].astype(BF16), w_out[...])
    out[...] = sums[:seqs] + first[...] * (1.0 / tp)


def second_body(seqs, s0, s1, s2, s3, rows, gate, up, down, keep, give, own_out, halves, sums_held):
    here, side = lax.axis_index("kv"), lax.axis_index("tp")
    count, _, width = halves.shape
    for peer, piece in zip(peers(here, side), (s0, s1, s2, s3)):
        piece = piece[...].astype(F32)
        halves[2 * peer] = piece[:, :width]
        halves[2 * peer + 1] = piece[:, width:]
    second = jnp.concatenate([halves[i] for i in range(count)], axis=1)
    padded = jnp.concatenate([second, second], axis=0)
    gain = rows[seqs + 2 : seqs + 3, :].astype(F32)
    sums = feed(normed_rows(padded, gain), 1, gate, up, down)[:seqs]
    for i in range(count):
        sums_held[i] = sums[:, i * width : (i + 1) * width]
    for out, core in ((keep, side), (give, 1 - side)):
        _, near, far, _ = peers(here, core)
        picks = (2 * far + core, 2 * far + 1 - core, 2 * near + core, 2 * here + core)
        for i, pick in enumerate(picks):
            out[:, i * width : (i + 1) * width] = sums_held[pick]
    own_out[...] = halves[2 * here + side]


def small_mesh(kv, tp, *args):
    return small_step(kv, tp, *args)


def small_step(
    kv,
    tp,
    resid,
    norm_gain,
    ffn_gate,
    ffn_up,
    ffn_down,
    w_x,
    w_z,
    w_bc,
    w_dt,
    dt_bias,
    a_log,
    d_skip,
    conv_wx,
    conv_wbc,
    conv_x,
    conv_bc,
    ssm_state,
    w_out,
):
    seqs, width = resid.shape
    model = width * kv * tp
    span = model // kv
    gate, up = jnp.swapaxes(ffn_gate, 1, 2), jnp.swapaxes(ffn_up, 1, 2)
    heads = dt_bias.shape[0]
    groups, states = w_bc.shape[2:]
    half = w_x.shape[2]
    local = w_x.shape[1] * half
    wide = heads // groups * half
    flat = heads * half

    pack = run(
        pack_body,
        bf16(2 * seqs, width),
        (in_hbm(resid), in_hbm(norm_gain)),
        [
            pltpu.VMEM(resid.shape, BF16),
            pltpu.VMEM(norm_gain.shape, BF16),
            pltpu.SemaphoreType.DMA((2,)),
        ],
        in_specs=[HBM] * 2,
    )
    chips = share_chip(jnp.concatenate([pack, swap_tp(pack)], axis=1))
    down = in_vmem(ffn_down)
    gate_one = turned_held(gate, 0)
    up_one = turned_held(up, 0)

    sums, rows = run(
        functools.partial(first_body, seqs),
        [f32(seqs, model), bf16(2 * seqs, model)],
        (*chips, gate_one, up_one, down),
        [pltpu.VMEM((kv * tp, 2 * seqs, width), BF16)],
    )
    sums = (sums + swap_tp(sums)).astype(BF16)
    sums = share_chip(sums)

    w_xs, w_zs = turned([jnp.transpose(w, (1, 2, 0)).reshape(local, model) for w in (w_x, w_z)])
    flat_bc = w_bc.reshape(span, 2 * groups * states)
    w_maps, w_steps, w_join = map(
        in_vmem,
        (
            flat_bc,
            w_dt.T,
            w_out.reshape(flat, span),
        ),
    )
    high, low = run(
        split_body, [bf16(flat, states)] * 2, (in_vmem(ssm_state.reshape(flat, states)),)
    )
    bc_width = 2 * groups * states
    line = 2 * local + bc_width + max(heads, 128)
    *pays, first = run(
        functools.partial(mix_in_body, kv, seqs),
        [f32(1, line)] * kv + [f32(seqs, span)],
        (*sums, rows, w_xs, w_zs, w_maps, w_steps),
        [
            pltpu.VMEM((kv, 2 * seqs, span), F32),
            pltpu.VMEM((kv, 2 * seqs, span), F32),
            pltpu.VMEM((2 * seqs, line), F32),
        ],
    )
    pays = swap_kv(pays)
    mixed = run(
        functools.partial(state_body, kv),
        f32(1, flat),
        (
            *pays,
            high,
            low,
            conv_wx.reshape(-1, groups, wide),
            conv_x.reshape(-1, groups, wide),
            conv_wbc.reshape(-1, 2 * groups, states),
            conv_bc.reshape(-1, 2 * groups, states),
            dt_bias.reshape(1, heads),
            a_log.reshape(1, heads),
            d_skip.reshape(1, heads),
        ),
        [
            pltpu.VMEM((groups, wide), F32),
            pltpu.VMEM((groups, wide), F32),
            pltpu.VMEM((2 * groups, states), F32),
        ],
    )
    mixed = share_kv(mixed, kv)
    joined = run(
        functools.partial(mix_out_body, seqs, tp),
        f32(seqs, span),
        (*mixed, w_join, first),
        [pltpu.VMEM((2 * seqs, flat), F32)],
    )
    second = share_chip((joined + swap_tp(joined)).astype(BF16))
    gate_two = turned_layer(gate, 1)
    up_two = turned_layer(up, 1)
    keep, give, base = run(
        functools.partial(second_body, seqs),
        [f32(seqs, 4 * width), f32(seqs, 4 * width), f32(seqs, width)],
        (*second, rows, gate_two, up_two, down),
        [pltpu.VMEM((kv * tp, seqs, width), F32), pltpu.VMEM((kv * tp, seqs, width), F32)],
    )
    total = keep + swap_tp(give)
    far = swap_far(total[:, : 2 * width])
    near = swap_near(total[:, 2 * width : 3 * width])
    rest = total[:, 3 * width :] + far[:, :width] + near + swap_tp(far[:, width:])
    return (base + 0.5 * rest).astype(BF16)


def normalize(rows, gain):
    values = rows.astype(jnp.float32)
    scale = lax.rsqrt(jnp.mean(values * values, axis=1, keepdims=True) + EPS)
    return (values * scale * gain.astype(jnp.float32).reshape(1, -1)).astype(jnp.bfloat16)


def feed_forward(normed, w_gate, w_up, w_down):
    gate = jnp.dot(normed, w_gate, preferred_element_type=jnp.float32)
    upper = jnp.dot(normed, w_up, preferred_element_type=jnp.float32)
    hidden = (jax.nn.silu(gate) * upper).astype(jnp.bfloat16)
    return jnp.dot(hidden, w_down, preferred_element_type=jnp.float32)


def add_half(base, sums):
    return (base.astype(jnp.float32) + 0.5 * sums).astype(jnp.bfloat16)


def ffn_totals(partial_value):
    return lax.psum(partial_value, ("kv", "tp"))


def short_conv(history, newest, taps):
    window = jnp.concatenate(
        [history.astype(jnp.float32), newest.astype(jnp.float32)[:, None]], axis=1
    )
    return jax.nn.silu(jnp.sum(window * taps.astype(jnp.float32)[None], axis=1))


def state_step(
    xs_new,
    zeta,
    bc_new,
    dt_raw,
    conv_x,
    conv_bc,
    ssm_state,
    conv_wx,
    conv_wbc,
    dt_bias,
    a_log,
    d_skip,
):
    xconv = short_conv(conv_x, xs_new, conv_wx)
    bconv = short_conv(conv_bc, bc_new, conv_wbc)
    heads = xconv.shape[1]
    groups = bconv.shape[2]
    bmat = jnp.repeat(bconv[:, 0], heads // groups, axis=1)
    cmat = jnp.repeat(bconv[:, 1], heads // groups, axis=1)
    step_size = jax.nn.softplus(dt_raw + dt_bias[None, :])
    decay = jnp.exp(-step_size * jnp.exp(a_log)[None, :])
    updated = (
        decay[:, :, None, None] * ssm_state
        + (step_size[:, :, None] * xconv)[..., None] * bmat[:, :, None, :]
    )
    mixed = (
        jnp.einsum("shpn,shn->shp", updated, cmat, precision=lax.Precision.HIGHEST)
        + d_skip[None, :, None] * xconv
    )
    return (mixed * jax.nn.silu(zeta.astype(jnp.float32))).astype(jnp.bfloat16)


def group_terms(slab, w_bc, w_dt):
    span = slab.shape[1]
    flat_bc = w_bc.reshape(span, -1)
    bc_part = jnp.dot(slab, flat_bc, preferred_element_type=jnp.float32)
    dt_part = jnp.dot(slab, w_dt, preferred_element_type=jnp.float32)
    return (
        lax.psum_scatter(bc_part, "kv", scatter_dimension=0, tiled=True),
        lax.psum_scatter(dt_part, "kv", scatter_dimension=0, tiled=True),
    )


def mix_partial(
    normed,
    w_x,
    w_z,
    w_bc,
    w_dt,
    dt_bias,
    a_log,
    d_skip,
    conv_wx,
    conv_wbc,
    conv_x,
    conv_bc,
    ssm_state,
    w_out,
):
    rows = normed.shape[0]
    local_heads = w_x.shape[1]
    half = w_x.shape[2]
    xs_part = (
        jnp.dot(normed, w_x.reshape(normed.shape[1], -1), preferred_element_type=jnp.float32)
        .astype(jnp.bfloat16)
        .reshape(rows, local_heads, half)
    )
    zeta_part = (
        jnp.dot(normed, w_z.reshape(normed.shape[1], -1), preferred_element_type=jnp.float32)
        .astype(jnp.bfloat16)
        .reshape(rows, local_heads, half)
    )
    xs_new, zeta = (
        lax.all_to_all(xs_part, "kv", split_axis=0, concat_axis=1, tiled=True),
        lax.all_to_all(zeta_part, "kv", split_axis=0, concat_axis=1, tiled=True),
    )
    span = w_bc.shape[0]
    slab = lax.dynamic_slice_in_dim(normed, lax.axis_index("kv") * span, span, 1)
    bc_sum, dt_raw = group_terms(slab, w_bc, w_dt)
    bc_new = bc_sum.astype(jnp.bfloat16).reshape((bc_sum.shape[0],) + w_bc.shape[1:])
    mixed = state_step(
        xs_new,
        zeta,
        bc_new,
        dt_raw,
        conv_x,
        conv_bc,
        ssm_state,
        conv_wx,
        conv_wbc,
        dt_bias,
        a_log,
        d_skip,
    )
    flat_out = w_out.reshape(-1, w_out.shape[2])
    piece = lax.all_gather(mixed, "kv", axis=0, tiled=True)
    return jnp.dot(piece.reshape(piece.shape[0], -1), flat_out, preferred_element_type=jnp.float32)


def per_device(
    resid,
    norm_gain,
    ffn_gate,
    ffn_up,
    ffn_down,
    w_x,
    w_z,
    w_bc,
    w_dt,
    dt_bias,
    a_log,
    d_skip,
    conv_wx,
    conv_wbc,
    conv_x,
    conv_bc,
    ssm_state,
    w_out,
):
    mixer_args = (
        w_x,
        w_z,
        w_bc,
        w_dt,
        dt_bias,
        a_log,
        d_skip,
        conv_wx,
        conv_wbc,
        conv_x,
        conv_bc,
        ssm_state,
        w_out,
    )
    rows, gains = (
        lax.all_gather(resid, ("kv", "tp"), axis=1, tiled=True),
        lax.all_gather(norm_gain, ("kv", "tp"), axis=1, tiled=True),
    )
    first = add_half(
        rows,
        ffn_totals(feed_forward(normalize(rows, gains[0]), ffn_gate[0], ffn_up[0], ffn_down[0])),
    )
    partial_value = mix_partial(normalize(first, gains[1]), *mixer_args)
    span = partial_value.shape[1]
    block = lax.dynamic_slice_in_dim(first, lax.axis_index("kv") * span, span, 1)
    joined = (block.astype(jnp.float32) + lax.psum(partial_value, "tp")).astype(jnp.bfloat16)
    second = lax.all_gather(joined, "kv", axis=1, tiled=True)
    final = add_half(
        second,
        ffn_totals(feed_forward(normalize(second, gains[2]), ffn_gate[1], ffn_up[1], ffn_down[1])),
    )
    width = resid.shape[1]
    return lax.dynamic_slice_in_dim(final, lax.axis_index(("kv", "tp")) * width, width, 1)


def solution(mesh):
    placed = (
        P("dp", ("kv", "tp")),
        P(None, ("kv", "tp")),
        P(None, None, ("kv", "tp")),
        P(None, None, ("kv", "tp")),
        P(None, ("kv", "tp"), None),
        P(None, "kv", "tp"),
        P(None, "kv", "tp"),
        P("kv", None, None, None),
        P("kv", None),
        P(),
        P(),
        P(),
        P(None, None, "tp"),
        P(),
        P(("dp", "kv"), None, None, "tp"),
        P(("dp", "kv"), None, None, None, None),
        P(("dp", "kv"), None, "tp", None),
        P(None, "tp", "kv"),
    )
    kv, tp = mesh.shape["kv"], mesh.shape["tp"]
    small = (kv, tp) == (4, 2)
    return jax.shard_map(
        functools.partial(small_mesh, kv, tp) if small else per_device,
        mesh=mesh,
        in_specs=placed,
        out_specs=P("dp", ("kv", "tp")),
        check_vma=False,
    )
```

```python
import functools

import jax
import jax.numpy as jnp
from jax import lax
from jax.experimental import pallas as pl
from jax.experimental.pallas import tpu as pltpu
from jax.sharding import PartitionSpec as P


EPS = 1e-06
F32 = jnp.float32
BF16 = jnp.bfloat16
NT = (((1,), (1,)), ((), ()))
HBM = pl.BlockSpec(memory_space=pltpu.HBM)
VMEM = pl.BlockSpec(memory_space=pltpu.VMEM)


def dot_nt(left, right):
    return lax.dot_general(left, right, NT, preferred_element_type=F32)


def dot_nn(left, right):
    return jnp.dot(left, right, preferred_element_type=F32)


def silu(value):
    return value * jax.nn.sigmoid(value)


def swap_kv(values):
    kv = len(values)
    got = list(values)
    for d in reversed(range(1, kv)):
        got[d] = lax.ppermute(values[d], "kv", [(i, i ^ d) for i in range(kv)])
    return got


def share_kv(value, kv):
    return swap_kv([value] * kv)


def swap_tp(value):
    return lax.ppermute(value, "tp", [(0, 1), (1, 0)])


def swap_far(value):
    pairs = [(2 * c + t, 2 * (c ^ (2 + t)) + t) for c in range(4) for t in range(2)]
    return lax.ppermute(value, ("kv", "tp"), pairs)


def swap_near(value):
    pairs = [(2 * c + t, 2 * (c ^ 1) + t) for c in range(4) for t in range(2)]
    return lax.ppermute(value, ("kv", "tp"), pairs)


def share_chip(value):
    far = swap_far(value)
    near = swap_near(value)
    return [value, near, far, swap_tp(far)]


def peers(here, side):
    return [jnp.bitwise_xor(here, d) for d in (0, 1, 2 + side, 3 - side)]


def in_vmem(value):
    return pltpu.with_memory_space_constraint(value, pltpu.VMEM)


def in_hbm(value):
    return pltpu.with_memory_space_constraint(value, pltpu.HBM)


def run(body, outs, args, scratch=(), limit=16, in_specs=None, flops=10**10):
    return pl.pallas_call(
        body,
        out_shape=outs,
        in_specs=in_specs or [VMEM] * len(args),
        out_specs=jax.tree.map(lambda _: VMEM, outs),
        scratch_shapes=list(scratch),
        compiler_params=pltpu.CompilerParams(vmem_limit_bytes=limit * 2**20),
        cost_estimate=pl.CostEstimate(flops=flops, bytes_accessed=0, transcendentals=0),
    )(*args)


def f32(*shape):
    return jax.ShapeDtypeStruct(shape, F32)


def bf16(*shape):
    return jax.ShapeDtypeStruct(shape, BF16)


def split_body(state, high_out, low_out):
    values = state[...]
    high = values.astype(BF16)
    high_out[...] = high
    low_out[...] = (values - high.astype(F32)).astype(BF16)


def normed_rows(values, gain):
    scale = lax.rsqrt(jnp.mean(values * values, axis=1, keepdims=True) + EPS)
    return (values * gain).astype(BF16), scale


def project(normed, layer, weights):
    if len(weights.shape) == 3:
        return dot_nt(normed, weights[layer])
    return dot_nn(normed, weights[...])


def feed(normed, scale, layer, gate, up, down):
    gated, upper = project(normed, layer, gate) * scale, project(normed, layer, up) * scale
    return dot_nn((silu(gated) * upper).astype(BF16), down[layer])


def pack_body(rows, gains, out, rows_held, gains_held, sems):
    copies = (
        pltpu.make_async_copy(rows, rows_held, sems.at[0]),
        pltpu.make_async_copy(gains, gains_held, sems.at[1]),
    )
    for copy in copies:
        copy.start()
    for copy in copies:
        copy.wait()
    seqs, count = rows_held.shape[0], gains_held.shape[0]
    out[:seqs] = rows_held[...]
    out[seqs : seqs + count] = gains_held[...]
    out[seqs + count :] = gains_held[:1]


def turn_body(*refs):
    count = len(refs) // 2
    for source, target in zip(refs[:count], refs[count:]):
        target[...] = source[...].T


def turned(sources):
    outs = run(
        turn_body, [bf16(*source.shape[::-1]) for source in sources], tuple(map(in_vmem, sources))
    )
    return [in_vmem(out) for out in outs]


TURN = 256


def turn_layer_body(layer, source, target, held, sems):
    height = held.shape[0]
    blocks = [pl.ds(i, min(TURN, height - i)) for i in range(0, height, TURN)]
    copies = [
        pltpu.make_async_copy(source.at[layer, rows], held.at[rows], sems.at[i])
        for i, rows in enumerate(blocks)
    ]
    for copy in copies:
        copy.start()
    for copy, rows in zip(copies, blocks):
        copy.wait()
        target[:, rows] = held[rows].T


def turn_held_body(layer, source, target):
    target[...] = source[layer].T


def turned_held(source, layer):
    out = run(
        functools.partial(turn_held_body, layer), bf16(*source.shape[:0:-1]), (in_vmem(source),)
    )
    return in_vmem(out)


def turned_layer(source, layer):
    height, wide = source.shape[1:]
    out = run(
        functools.partial(turn_layer_body, layer),
        bf16(wide, height),
        (in_hbm(source),),
        [
            pltpu.VMEM((height, wide), BF16),
            pltpu.SemaphoreType.DMA((pl.cdiv(height, TURN),)),
        ],
        in_specs=[HBM],
    )
    return in_vmem(out)


def first_body(seqs, c0, c1, c2, c3, gate, up, down, sums_out, rows_out, slabs):
    here, side = lax.axis_index("kv"), lax.axis_index("tp")
    width = slabs.shape[2]
    for peer, piece, first in zip(peers(here, side), (c0, c1, c2, c3), (side, side, side, 1 - side)):
        slabs[2 * peer + first] = piece[:, :width]
        slabs[2 * peer + 1 - first] = piece[:, width:]
    rows = jnp.concatenate([slabs[i] for i in range(slabs.shape[0])], axis=1)
    rows_out[...] = rows
    values = rows.astype(F32)
    sums = feed(*normed_rows(values, values[seqs : seqs + 1]), 0, gate, up, down)
    sums_out[...] = sums[:seqs]


def mix_in_body(kv, seqs, s0, s1, s2, s3, rows, w_x, w_z, w_bc, w_dt, *rest):
    pays, (first_out, slabs, firsts, table) = rest[:kv], rest[kv:]
    here = lax.axis_index("kv")
    span = slabs.shape[2]
    total = s0[...].astype(F32) + s1[...].astype(F32) + s2[...].astype(F32) + s3[...].astype(F32)
    known = rows[...].astype(F32)
    first = (known[:seqs] + 0.5 * total).astype(BF16).astype(F32)
    padded = jnp.concatenate([first, first], axis=0)
    normed, scale = normed_rows(padded, known[seqs + 1 : seqs + 2])
    for i in range(kv):
        slabs[i] = normed[:, i * span : (i + 1) * span].astype(F32)
        firsts[i] = padded[:, i * span : (i + 1) * span]
    slab = slabs[here].astype(BF16)
    first_out[...] = firsts[here][:seqs]
    xs = (dot_nn(normed, w_x[...]) * scale).astype(BF16).astype(F32)
    zeta = (dot_nn(normed, w_z[...]) * scale).astype(BF16).astype(F32)
    bc = dot_nn(slab, w_bc[...]) * scale
    dt = dot_nt(slab, w_dt[...]) * scale
    width = xs.shape[1]
    a = 2 * width
    b = a + bc.shape[1]
    table[:, :width] = xs
    table[:, width:a] = zeta
    table[:, a:b] = bc
    table[:, b : b + dt.shape[1]] = dt
    for d in range(kv):
        pays[d][...] = table[pl.ds(jnp.bitwise_xor(here, d), 1), :]


def state_body(kv, p0, p1, p2, p3, high, low, taps_x, past_x, taps_bc, past_bc, bias, a_log, d_skip, out, x_held, z_held, bc_held):
    here = lax.axis_index("kv")
    groups, wide = x_held.shape
    states = bc_held.shape[1]
    heads = bias.shape[1]
    pieces = (p0, p1, p2, p3)
    per = groups // kv
    width = per * wide
    for d, piece in enumerate(pieces):
        peer = jnp.bitwise_xor(here, d)
        for i in range(per):
            x_held[pl.ds(per * peer + i, 1), :] = piece[:, i * wide : (i + 1) * wide]
            z_held[pl.ds(per * peer + i, 1), :] = piece[:, width + i * wide : width + (i + 1) * wide]
    a = 2 * width
    for j in range(2 * groups):
        at = a + j * states
        bc_held[j : j + 1, :] = sum(piece[:, at : at + states] for piece in pieces)
    b = a + 2 * groups * states
    dt = sum(piece[:, b : b + heads] for piece in pieces) + bias[...]
    newest = bc_held[...].astype(BF16).astype(F32)
    steps = taps_bc.shape[0]
    mapped = newest * taps_bc[steps - 1].astype(F32)
    for k in range(steps - 1):
        mapped += past_bc[k].astype(F32) * taps_bc[k].astype(F32)
    mapped = silu(mapped)
    b_map, c_map = mapped[:groups], mapped[groups:]
    xconv = x_held[...] * taps_x[steps - 1].astype(F32)
    for k in range(steps - 1):
        xconv += past_x[k].astype(F32) * taps_x[k].astype(F32)
    xconv = silu(xconv)
    share = heads // groups
    own_group = lax.broadcasted_iota(jnp.int32, (groups, heads), 1) // share == lax.broadcasted_iota(
        jnp.int32, (groups, heads), 0
    )
    spread = (
        lax.broadcasted_iota(jnp.int32, (heads, wide), 0) % share
        == lax.broadcasted_iota(jnp.int32, (heads, wide), 1) // (wide // share)
    ).astype(F32)
    table = jnp.concatenate(
        [
            jnp.where(own_group, jnp.broadcast_to(v, (groups, heads)), 0.0)
            for v in (dt, a_log[...], d_skip[...])
        ],
        axis=0,
    )
    table = jnp.dot(table, spread, precision=lax.Precision.HIGHEST, preferred_element_type=F32)
    step = jax.nn.softplus(table[:groups])
    decay = jnp.exp(-step * jnp.exp(table[groups : 2 * groups]))
    skip = table[2 * groups :]
    c_high = c_map.astype(BF16)
    c_low = (c_map - c_high.astype(F32)).astype(BF16)
    read = dot_nt(c_high, high[...]) + dot_nt(c_low, high[...]) + dot_nt(c_high, low[...])
    read = jnp.concatenate(
        [read[g : g + 1, g * wide : (g + 1) * wide] for g in range(groups)], axis=0
    )
    inner = jnp.sum(b_map * c_map, axis=1, keepdims=True)
    mixed = (decay * read + xconv * (step * inner + skip)) * silu(z_held[...])
    mixed = mixed.astype(BF16).astype(F32)
    for g in range(groups):
        out[:, g * wide : (g + 1) * wide] = mixed[g : g + 1]


def mix_out_body(seqs, tp, m0, m1, m2, m3, w_out, first, out, table):
    here = lax.axis_index("kv")
    table[...] = jnp.zeros_like(table)
    for d, piece in enumerate((m0, m1, m2, m3)):
        table[pl.ds(jnp.bitwise_xor(here, d), 1), :] = piece[...]
    sums = dot_nn(table[...].astype(BF16), w_out[...])
    out[...] = sums[:seqs] + first[...] * (1.0 / tp)


def second_body(seqs, s0, s1, s2, s3, rows, gate, up, down, keep, give, own_out, halves, sums_held):
    here, side = lax.axis_index("kv"), lax.axis_index("tp")
    count, _, width = halves.shape
    for peer, piece in zip(peers(here, side), (s0, s1, s2, s3)):
        piece = piece[...].astype(F32)
        halves[2 * peer] = piece[:, :width]
        halves[2 * peer + 1] = piece[:, width:]
    second = jnp.concatenate([halves[i] for i in range(count)], axis=1)
    padded = jnp.concatenate([second, second], axis=0)
    gain = rows[seqs + 2 : seqs + 3, :].astype(F32)
    sums = feed(*normed_rows(padded, gain), 1, gate, up, down)[:seqs]
    for i in range(count):
        sums_held[i] = sums[:, i * width : (i + 1) * width]
    for out, core in ((keep, side), (give, 1 - side)):
        _, near, far, _ = peers(here, core)
        picks = (2 * far + core, 2 * far + 1 - core, 2 * near + core, 2 * here + core)
        for i, pick in enumerate(picks):
            out[:, i * width : (i + 1) * width] = sums_held[pick]
    own_out[...] = halves[2 * here + side]


def small_mesh(kv, tp, *args):
    return small_step(kv, tp, *args)


def small_step(
    kv,
    tp,
    resid,
    norm_gain,
    ffn_gate,
    ffn_up,
    ffn_down,
    w_x,
    w_z,
    w_bc,
    w_dt,
    dt_bias,
    a_log,
    d_skip,
    conv_wx,
    conv_wbc,
    conv_x,
    conv_bc,
    ssm_state,
    w_out,
):
    seqs, width = resid.shape
    model = width * kv * tp
    span = model // kv
    gate, up = jnp.swapaxes(ffn_gate, 1, 2), jnp.swapaxes(ffn_up, 1, 2)
    heads = dt_bias.shape[0]
    groups, states = w_bc.shape[2:]
    half = w_x.shape[2]
    local = w_x.shape[1] * half
    wide = heads // groups * half
    flat = heads * half

    pack = run(
        pack_body,
        bf16(2 * seqs, width),
        (in_hbm(resid), in_hbm(norm_gain)),
        [
            pltpu.VMEM(resid.shape, BF16),
            pltpu.VMEM(norm_gain.shape, BF16),
            pltpu.SemaphoreType.DMA((2,)),
        ],
        in_specs=[HBM] * 2,
    )
    chips = share_chip(jnp.concatenate([pack, swap_tp(pack)], axis=1))
    down = in_vmem(ffn_down)
    gate_one = turned_held(gate, 0)
    up_one = turned_held(up, 0)

    sums, rows = run(
        functools.partial(first_body, seqs),
        [f32(seqs, model), bf16(2 * seqs, model)],
        (*chips, gate_one, up_one, down),
        [pltpu.VMEM((kv * tp, 2 * seqs, width), BF16)],
    )
    sums = (sums + swap_tp(sums)).astype(BF16)
    sums = share_chip(sums)

    w_xs, w_zs = turned([jnp.transpose(w, (1, 2, 0)).reshape(local, model) for w in (w_x, w_z)])
    flat_bc = w_bc.reshape(span, 2 * groups * states)
    w_maps, w_steps, w_join = map(
        in_vmem,
        (
            flat_bc,
            w_dt.T,
            w_out.reshape(flat, span),
        ),
    )
    high, low = run(
        split_body, [bf16(flat, states)] * 2, (in_vmem(ssm_state.reshape(flat, states)),)
    )
    bc_width = 2 * groups * states
    line = 2 * local + bc_width + max(heads, 128)
    *pays, first = run(
        functools.partial(mix_in_body, kv, seqs),
        [f32(1, line)] * kv + [f32(seqs, span)],
        (*sums, rows, w_xs, w_zs, w_maps, w_steps),
        [
            pltpu.VMEM((kv, 2 * seqs, span), F32),
            pltpu.VMEM((kv, 2 * seqs, span), F32),
            pltpu.VMEM((2 * seqs, line), F32),
        ],
    )
    pays = swap_kv(pays)
    mixed = run(
        functools.partial(state_body, kv),
        f32(1, flat),
        (
            *pays,
            high,
            low,
            conv_wx.reshape(-1, groups, wide),
            conv_x.reshape(-1, groups, wide),
            conv_wbc.reshape(-1, 2 * groups, states),
            conv_bc.reshape(-1, 2 * groups, states),
            dt_bias.reshape(1, heads),
            a_log.reshape(1, heads),
            d_skip.reshape(1, heads),
        ),
        [
            pltpu.VMEM((groups, wide), F32),
            pltpu.VMEM((groups, wide), F32),
            pltpu.VMEM((2 * groups, states), F32),
        ],
    )
    mixed = share_kv(mixed, kv)
    joined = run(
        functools.partial(mix_out_body, seqs, tp),
        f32(seqs, span),
        (*mixed, w_join, first),
        [pltpu.VMEM((2 * seqs, flat), F32)],
    )
    second = share_chip((joined + swap_tp(joined)).astype(BF16))
    gate_two = turned_layer(gate, 1)
    up_two = turned_layer(up, 1)
    keep, give, base = run(
        functools.partial(second_body, seqs),
        [f32(seqs, 4 * width), f32(seqs, 4 * width), f32(seqs, width)],
        (*second, rows, gate_two, up_two, down),
        [pltpu.VMEM((kv * tp, seqs, width), F32), pltpu.VMEM((kv * tp, seqs, width), F32)],
    )
    total = keep + swap_tp(give)
    far = swap_far(total[:, : 2 * width])
    near = swap_near(total[:, 2 * width : 3 * width])
    rest = total[:, 3 * width :] + far[:, :width] + near + swap_tp(far[:, width:])
    return (base + 0.5 * rest).astype(BF16)


def normalize(rows, gain):
    values = rows.astype(jnp.float32)
    scale = lax.rsqrt(jnp.mean(values * values, axis=1, keepdims=True) + EPS)
    return (values * scale * gain.astype(jnp.float32).reshape(1, -1)).astype(jnp.bfloat16)


def feed_forward(normed, w_gate, w_up, w_down):
    gate = jnp.dot(normed, w_gate, preferred_element_type=jnp.float32)
    upper = jnp.dot(normed, w_up, preferred_element_type=jnp.float32)
    hidden = (jax.nn.silu(gate) * upper).astype(jnp.bfloat16)
    return jnp.dot(hidden, w_down, preferred_element_type=jnp.float32)


def add_half(base, sums):
    return (base.astype(jnp.float32) + 0.5 * sums).astype(jnp.bfloat16)


def ffn_totals(partial_value):
    return lax.psum(partial_value, ("kv", "tp"))


def short_conv(history, newest, taps):
    window = jnp.concatenate(
        [history.astype(jnp.float32), newest.astype(jnp.float32)[:, None]], axis=1
    )
    return jax.nn.silu(jnp.sum(window * taps.astype(jnp.float32)[None], axis=1))


def state_step(
    xs_new,
    zeta,
    bc_new,
    dt_raw,
    conv_x,
    conv_bc,
    ssm_state,
    conv_wx,
    conv_wbc,
    dt_bias,
    a_log,
    d_skip,
):
    xconv = short_conv(conv_x, xs_new, conv_wx)
    bconv = short_conv(conv_bc, bc_new, conv_wbc)
    heads = xconv.shape[1]
    groups = bconv.shape[2]
    bmat = jnp.repeat(bconv[:, 0], heads // groups, axis=1)
    cmat = jnp.repeat(bconv[:, 1], heads // groups, axis=1)
    step_size = jax.nn.softplus(dt_raw + dt_bias[None, :])
    decay = jnp.exp(-step_size * jnp.exp(a_log)[None, :])
    updated = (
        decay[:, :, None, None] * ssm_state
        + (step_size[:, :, None] * xconv)[..., None] * bmat[:, :, None, :]
    )
    mixed = (
        jnp.einsum("shpn,shn->shp", updated, cmat, precision=lax.Precision.HIGHEST)
        + d_skip[None, :, None] * xconv
    )
    return (mixed * jax.nn.silu(zeta.astype(jnp.float32))).astype(jnp.bfloat16)


def group_terms(slab, w_bc, w_dt):
    span = slab.shape[1]
    flat_bc = w_bc.reshape(span, -1)
    bc_part = jnp.dot(slab, flat_bc, preferred_element_type=jnp.float32)
    dt_part = jnp.dot(slab, w_dt, preferred_element_type=jnp.float32)
    return (
        lax.psum_scatter(bc_part, "kv", scatter_dimension=0, tiled=True),
        lax.psum_scatter(dt_part, "kv", scatter_dimension=0, tiled=True),
    )


def mix_partial(
    normed,
    w_x,
    w_z,
    w_bc,
    w_dt,
    dt_bias,
    a_log,
    d_skip,
    conv_wx,
    conv_wbc,
    conv_x,
    conv_bc,
    ssm_state,
    w_out,
):
    rows = normed.shape[0]
    local_heads = w_x.shape[1]
    half = w_x.shape[2]
    xs_part = (
        jnp.dot(normed, w_x.reshape(normed.shape[1], -1), preferred_element_type=jnp.float32)
        .astype(jnp.bfloat16)
        .reshape(rows, local_heads, half)
    )
    zeta_part = (
        jnp.dot(normed, w_z.reshape(normed.shape[1], -1), preferred_element_type=jnp.float32)
        .astype(jnp.bfloat16)
        .reshape(rows, local_heads, half)
    )
    xs_new, zeta = (
        lax.all_to_all(xs_part, "kv", split_axis=0, concat_axis=1, tiled=True),
        lax.all_to_all(zeta_part, "kv", split_axis=0, concat_axis=1, tiled=True),
    )
    span = w_bc.shape[0]
    slab = lax.dynamic_slice_in_dim(normed, lax.axis_index("kv") * span, span, 1)
    bc_sum, dt_raw = group_terms(slab, w_bc, w_dt)
    bc_new = bc_sum.astype(jnp.bfloat16).reshape((bc_sum.shape[0],) + w_bc.shape[1:])
    mixed = state_step(
        xs_new,
        zeta,
        bc_new,
        dt_raw,
        conv_x,
        conv_bc,
        ssm_state,
        conv_wx,
        conv_wbc,
        dt_bias,
        a_log,
        d_skip,
    )
    flat_out = w_out.reshape(-1, w_out.shape[2])
    piece = lax.all_gather(mixed, "kv", axis=0, tiled=True)
    return jnp.dot(piece.reshape(piece.shape[0], -1), flat_out, preferred_element_type=jnp.float32)


def per_device(
    resid,
    norm_gain,
    ffn_gate,
    ffn_up,
    ffn_down,
    w_x,
    w_z,
    w_bc,
    w_dt,
    dt_bias,
    a_log,
    d_skip,
    conv_wx,
    conv_wbc,
    conv_x,
    conv_bc,
    ssm_state,
    w_out,
):
    mixer_args = (
        w_x,
        w_z,
        w_bc,
        w_dt,
        dt_bias,
        a_log,
        d_skip,
        conv_wx,
        conv_wbc,
        conv_x,
        conv_bc,
        ssm_state,
        w_out,
    )
    rows, gains = (
        lax.all_gather(resid, ("kv", "tp"), axis=1, tiled=True),
        lax.all_gather(norm_gain, ("kv", "tp"), axis=1, tiled=True),
    )
    first = add_half(
        rows,
        ffn_totals(feed_forward(normalize(rows, gains[0]), ffn_gate[0], ffn_up[0], ffn_down[0])),
    )
    partial_value = mix_partial(normalize(first, gains[1]), *mixer_args)
    span = partial_value.shape[1]
    block = lax.dynamic_slice_in_dim(first, lax.axis_index("kv") * span, span, 1)
    joined = (block.astype(jnp.float32) + lax.psum(partial_value, "tp")).astype(jnp.bfloat16)
    second = lax.all_gather(joined, "kv", axis=1, tiled=True)
    final = add_half(
        second,
        ffn_totals(feed_forward(normalize(second, gains[2]), ffn_gate[1], ffn_up[1], ffn_down[1])),
    )
    width = resid.shape[1]
    return lax.dynamic_slice_in_dim(final, lax.axis_index(("kv", "tp")) * width, width, 1)


def solution(mesh):
    placed = (
        P("dp", ("kv", "tp")),
        P(None, ("kv", "tp")),
        P(None, None, ("kv", "tp")),
        P(None, None, ("kv", "tp")),
        P(None, ("kv", "tp"), None),
        P(None, "kv", "tp"),
        P(None, "kv", "tp"),
        P("kv", None, None, None),
        P("kv", None),
        P(),
        P(),
        P(),
        P(None, None, "tp"),
        P(),
        P(("dp", "kv"), None, None, "tp"),
        P(("dp", "kv"), None, None, None, None),
        P(("dp", "kv"), None, "tp", None),
        P(None, "tp", "kv"),
    )
    kv, tp = mesh.shape["kv"], mesh.shape["tp"]
    small = (kv, tp) == (4, 2)
    return jax.shard_map(
        functools.partial(small_mesh, kv, tp) if small else per_device,
        mesh=mesh,
        in_specs=placed,
        out_specs=P("dp", ("kv", "tp")),
        check_vma=False,
    )
```

```python
import functools

import jax
import jax.numpy as jnp
from jax import lax
from jax.experimental import pallas as pl
from jax.experimental.pallas import tpu as pltpu
from jax.sharding import PartitionSpec as P


EPS = 1e-06
F32 = jnp.float32
BF16 = jnp.bfloat16
NT = (((1,), (1,)), ((), ()))
HBM = pl.BlockSpec(memory_space=pltpu.HBM)
VMEM = pl.BlockSpec(memory_space=pltpu.VMEM)


def dot_nt(left, right):
    return lax.dot_general(left, right, NT, preferred_element_type=F32)


def dot_nn(left, right):
    return jnp.dot(left, right, preferred_element_type=F32)


def silu(value):
    return value * jax.nn.sigmoid(value)


def swap_kv(values):
    kv = len(values)
    got = list(values)
    for d in reversed(range(1, kv)):
        got[d] = lax.ppermute(values[d], "kv", [(i, i ^ d) for i in range(kv)])
    return got


def share_kv(value, kv):
    return swap_kv([value] * kv)


def swap_tp(value):
    return lax.ppermute(value, "tp", [(0, 1), (1, 0)])


def swap_far(value):
    pairs = [(2 * c + t, 2 * (c ^ (2 + t)) + t) for c in range(4) for t in range(2)]
    return lax.ppermute(value, ("kv", "tp"), pairs)


def swap_near(value):
    pairs = [(2 * c + t, 2 * (c ^ 1) + t) for c in range(4) for t in range(2)]
    return lax.ppermute(value, ("kv", "tp"), pairs)


def share_chip(value):
    far = swap_far(value)
    near = swap_near(value)
    return [value, near, far, swap_tp(far)]


def peers(here, side):
    return [jnp.bitwise_xor(here, d) for d in (0, 1, 2 + side, 3 - side)]


def in_vmem(value):
    return pltpu.with_memory_space_constraint(value, pltpu.VMEM)


def in_hbm(value):
    return pltpu.with_memory_space_constraint(value, pltpu.HBM)


def run(body, outs, args, scratch=(), limit=16, in_specs=None, flops=10**10):
    return pl.pallas_call(
        body,
        out_shape=outs,
        in_specs=in_specs or [VMEM] * len(args),
        out_specs=jax.tree.map(lambda _: VMEM, outs),
        scratch_shapes=list(scratch),
        compiler_params=pltpu.CompilerParams(vmem_limit_bytes=limit * 2**20),
        cost_estimate=pl.CostEstimate(flops=flops, bytes_accessed=0, transcendentals=0),
    )(*args)


def f32(*shape):
    return jax.ShapeDtypeStruct(shape, F32)


def bf16(*shape):
    return jax.ShapeDtypeStruct(shape, BF16)


def split_body(state, high_out, low_out):
    values = state[...]
    high = values.astype(BF16)
    high_out[...] = high
    low_out[...] = (values - high.astype(F32)).astype(BF16)


def normed_rows(values, gain):
    scale = lax.rsqrt(jnp.mean(values * values, axis=1, keepdims=True) + EPS)
    return (values * gain).astype(BF16), scale


def project(normed, layer, weights):
    if len(weights.shape) == 3:
        return dot_nt(normed, weights[layer])
    return dot_nn(normed, weights[...])


def feed(normed, scale, layer, gate, up, down):
    gated, upper = project(normed, layer, gate) * scale, project(normed, layer, up) * scale
    return dot_nn((silu(gated) * upper).astype(BF16), down[layer])


def pack_body(rows, gains, out, rows_held, gains_held, sems):
    copies = (
        pltpu.make_async_copy(rows, rows_held, sems.at[0]),
        pltpu.make_async_copy(gains, gains_held, sems.at[1]),
    )
    for copy in copies:
        copy.start()
    for copy in copies:
        copy.wait()
    seqs, count = rows_held.shape[0], gains_held.shape[0]
    out[:seqs] = rows_held[...]
    out[seqs : seqs + count] = gains_held[...]
    out[seqs + count :] = gains_held[:1]


def turn_body(*refs):
    count = len(refs) // 2
    for source, target in zip(refs[:count], refs[count:]):
        target[...] = source[...].T


def turned(sources):
    outs = run(
        turn_body, [bf16(*source.shape[::-1]) for source in sources], tuple(map(in_vmem, sources))
    )
    return [in_vmem(out) for out in outs]


TURN = 256


def turn_layer_body(layer, source, target, held, sems):
    height = held.shape[0]
    blocks = [pl.ds(i, min(TURN, height - i)) for i in range(0, height, TURN)]
    copies = [
        pltpu.make_async_copy(source.at[layer, rows], held.at[rows], sems.at[i])
        for i, rows in enumerate(blocks)
    ]
    for copy in copies:
        copy.start()
    for copy, rows in zip(copies, blocks):
        copy.wait()
        target[:, rows] = held[rows].T


def turn_held_body(layer, source, target):
    target[...] = source[layer].T


def turned_held(source, layer):
    out = run(
        functools.partial(turn_held_body, layer), bf16(*source.shape[:0:-1]), (in_vmem(source),)
    )
    return in_vmem(out)


def turned_layer(source, layer):
    height, wide = source.shape[1:]
    out = run(
        functools.partial(turn_layer_body, layer),
        bf16(wide, height),
        (in_hbm(source),),
        [
            pltpu.VMEM((height, wide), BF16),
            pltpu.SemaphoreType.DMA((pl.cdiv(height, TURN),)),
        ],
        in_specs=[HBM],
    )
    return in_vmem(out)


def first_body(seqs, c0, c1, c2, c3, gate, up, down, sums_out, rows_out, slabs):
    here, side = lax.axis_index("kv"), lax.axis_index("tp")
    width = slabs.shape[2]
    for peer, piece, first in zip(peers(here, side), (c0, c1, c2, c3), (side, side, side, 1 - side)):
        slabs[2 * peer + first] = piece[:, :width]
        slabs[2 * peer + 1 - first] = piece[:, width:]
    rows = jnp.concatenate([slabs[i] for i in range(slabs.shape[0])], axis=1)
    rows_out[...] = rows
    values = rows.astype(F32)
    sums = feed(*normed_rows(values, values[seqs : seqs + 1]), 0, gate, up, down)
    sums_out[...] = sums[:seqs]


def mix_in_body(kv, seqs, s0, s1, s2, s3, rows, w_x, w_z, w_bc, w_dt, *rest):
    pays, (first_out, slabs, firsts, table) = rest[:kv], rest[kv:]
    here = lax.axis_index("kv")
    span = slabs.shape[2]
    total = s0[...].astype(F32) + s1[...].astype(F32) + s2[...].astype(F32) + s3[...].astype(F32)
    known = rows[...].astype(F32)
    first = (known[:seqs] + 0.5 * total).astype(BF16).astype(F32)
    padded = jnp.concatenate([first, first], axis=0)
    normed, scale = normed_rows(padded, known[seqs + 1 : seqs + 2])
    for i in range(kv):
        slabs[i] = normed[:, i * span : (i + 1) * span].astype(F32)
        firsts[i] = padded[:, i * span : (i + 1) * span]
    slab = slabs[here].astype(BF16)
    first_out[...] = firsts[here][:seqs]
    xs = (dot_nn(normed, w_x[...]) * scale).astype(BF16).astype(F32)
    zeta = (dot_nn(normed, w_z[...]) * scale).astype(BF16).astype(F32)
    bc = dot_nn(slab, w_bc[...]) * scale
    dt = dot_nt(slab, w_dt[...]) * scale
    width = xs.shape[1]
    a = 2 * width
    b = a + bc.shape[1]
    table[:, :width] = xs
    table[:, width:a] = zeta
    table[:, a:b] = bc
    table[:, b : b + dt.shape[1]] = dt
    for d in range(kv):
        pays[d][...] = table[pl.ds(jnp.bitwise_xor(here, d), 1), :]


def state_body(kv, p0, p1, p2, p3, high, low, taps_x, past_x, taps_bc, past_bc, bias, a_log, d_skip, out, x_held, z_held, bc_held):
    here = lax.axis_index("kv")
    groups, wide = x_held.shape
    states = bc_held.shape[1]
    heads = bias.shape[1]
    pieces = (p0, p1, p2, p3)
    per = groups // kv
    width = per * wide
    for d, piece in enumerate(pieces):
        peer = jnp.bitwise_xor(here, d)
        for i in range(per):
            x_held[pl.ds(per * peer + i, 1), :] = piece[:, i * wide : (i + 1) * wide]
            z_held[pl.ds(per * peer + i, 1), :] = piece[:, width + i * wide : width + (i + 1) * wide]
    a = 2 * width
    for j in range(2 * groups):
        at = a + j * states
        bc_held[j : j + 1, :] = sum(piece[:, at : at + states] for piece in pieces)
    b = a + 2 * groups * states
    dt = sum(piece[:, b : b + heads] for piece in pieces) + bias[...]
    newest = bc_held[...].astype(BF16).astype(F32)
    steps = taps_bc.shape[0]
    mapped = newest * taps_bc[steps - 1].astype(F32)
    for k in range(steps - 1):
        mapped += past_bc[k].astype(F32) * taps_bc[k].astype(F32)
    mapped = silu(mapped)
    b_map, c_map = mapped[:groups], mapped[groups:]
    xconv = x_held[...] * taps_x[steps - 1].astype(F32)
    for k in range(steps - 1):
        xconv += past_x[k].astype(F32) * taps_x[k].astype(F32)
    xconv = silu(xconv)
    share = heads // groups
    own_group = lax.broadcasted_iota(jnp.int32, (groups, heads), 1) // share == lax.broadcasted_iota(
        jnp.int32, (groups, heads), 0
    )
    spread = (
        lax.broadcasted_iota(jnp.int32, (heads, wide), 0) % share
        == lax.broadcasted_iota(jnp.int32, (heads, wide), 1) // (wide // share)
    ).astype(F32)
    table = jnp.concatenate(
        [
            jnp.where(own_group, jnp.broadcast_to(v, (groups, heads)), 0.0)
            for v in (dt, a_log[...], d_skip[...])
        ],
        axis=0,
    )
    table = jnp.dot(table, spread, precision=lax.Precision.HIGHEST, preferred_element_type=F32)
    step = jax.nn.softplus(table[:groups])
    decay = jnp.exp(-step * jnp.exp(table[groups : 2 * groups]))
    skip = table[2 * groups :]
    c_high = c_map.astype(BF16)
    c_low = (c_map - c_high.astype(F32)).astype(BF16)
    read = dot_nt(c_high, high[...]) + dot_nt(c_low, high[...]) + dot_nt(c_high, low[...])
    read = jnp.concatenate(
        [read[g : g + 1, g * wide : (g + 1) * wide] for g in range(groups)], axis=0
    )
    inner = jnp.sum(b_map * c_map, axis=1, keepdims=True)
    mixed = (decay * read + xconv * (step * inner + skip)) * silu(z_held[...])
    mixed = mixed.astype(BF16).astype(F32)
    for g in range(groups):
        out[:, g * wide : (g + 1) * wide] = mixed[g : g + 1]


def mix_out_body(seqs, tp, m0, m1, m2, m3, w_out, first, out, table):
    here = lax.axis_index("kv")
    table[...] = jnp.zeros_like(table)
    for d, piece in enumerate((m0, m1, m2, m3)):
        table[pl.ds(jnp.bitwise_xor(here, d), 1), :] = piece[...]
    sums = dot_nn(table[...].astype(BF16), w_out[...])
    out[...] = sums[:seqs] + first[...] * (1.0 / tp)


def second_body(seqs, s0, s1, s2, s3, rows, gate, up, down, keep, give, own_out, halves, sums_held):
    here, side = lax.axis_index("kv"), lax.axis_index("tp")
    count, _, width = halves.shape
    for peer, piece in zip(peers(here, side), (s0, s1, s2, s3)):
        piece = piece[...].astype(F32)
        halves[2 * peer] = piece[:, :width]
        halves[2 * peer + 1] = piece[:, width:]
    second = jnp.concatenate([halves[i] for i in range(count)], axis=1)
    padded = jnp.concatenate([second, second], axis=0)
    gain = rows[seqs + 2 : seqs + 3, :].astype(F32)
    sums = feed(*normed_rows(padded, gain), 1, gate, up, down)[:seqs]
    for i in range(count):
        sums_held[i] = sums[:, i * width : (i + 1) * width]
    for out, core in ((keep, side), (give, 1 - side)):
        _, near, far, _ = peers(here, core)
        picks = (2 * far + core, 2 * far + 1 - core, 2 * near + core, 2 * here + core)
        for i, pick in enumerate(picks):
            out[:, i * width : (i + 1) * width] = sums_held[pick]
    own_out[...] = halves[2 * here + side]


def small_mesh(kv, tp, *args):
    return small_step(kv, tp, *args)


def small_step(
    kv,
    tp,
    resid,
    norm_gain,
    ffn_gate,
    ffn_up,
    ffn_down,
    w_x,
    w_z,
    w_bc,
    w_dt,
    dt_bias,
    a_log,
    d_skip,
    conv_wx,
    conv_wbc,
    conv_x,
    conv_bc,
    ssm_state,
    w_out,
):
    seqs, width = resid.shape
    model = width * kv * tp
    span = model // kv
    gate, up = jnp.swapaxes(ffn_gate, 1, 2), jnp.swapaxes(ffn_up, 1, 2)
    heads = dt_bias.shape[0]
    groups, states = w_bc.shape[2:]
    half = w_x.shape[2]
    local = w_x.shape[1] * half
    wide = heads // groups * half
    flat = heads * half

    pack = run(
        pack_body,
        bf16(2 * seqs, width),
        (in_hbm(resid), in_hbm(norm_gain)),
        [
            pltpu.VMEM(resid.shape, BF16),
            pltpu.VMEM(norm_gain.shape, BF16),
            pltpu.SemaphoreType.DMA((2,)),
        ],
        in_specs=[HBM] * 2,
    )
    chips = share_chip(jnp.concatenate([pack, swap_tp(pack)], axis=1))
    down = in_vmem(ffn_down)
    gate_one = turned_held(gate, 0)
    up_one = turned_held(up, 0)

    sums, rows = run(
        functools.partial(first_body, seqs),
        [f32(seqs, model), bf16(2 * seqs, model)],
        (*chips, gate_one, up_one, down),
        [pltpu.VMEM((kv * tp, 2 * seqs, width), BF16)],
    )
    sums = (sums + swap_tp(sums)).astype(BF16)
    sums = share_chip(sums)

    w_xs, w_zs = turned([jnp.transpose(w, (1, 2, 0)).reshape(local, model) for w in (w_x, w_z)])
    flat_bc = w_bc.reshape(span, 2 * groups * states)
    w_maps, w_steps, w_join = map(
        in_vmem,
        (
            flat_bc,
            w_dt.T,
            w_out.reshape(flat, span),
        ),
    )
    high, low = run(
        split_body, [bf16(flat, states)] * 2, (in_vmem(ssm_state.reshape(flat, states)),)
    )
    bc_width = 2 * groups * states
    line = 2 * local + bc_width + max(heads, 128)
    *pays, first = run(
        functools.partial(mix_in_body, kv, seqs),
        [f32(1, line)] * kv + [f32(seqs, span)],
        (*sums, rows, w_xs, w_zs, w_maps, w_steps),
        [
            pltpu.VMEM((kv, 2 * seqs, span), F32),
            pltpu.VMEM((kv, 2 * seqs, span), F32),
            pltpu.VMEM((2 * seqs, line), F32),
        ],
    )
    pays = swap_kv(pays)
    mixed = run(
        functools.partial(state_body, kv),
        f32(1, flat),
        (
            *pays,
            high,
            low,
            conv_wx.reshape(-1, groups, wide),
            conv_x.reshape(-1, groups, wide),
            conv_wbc.reshape(-1, 2 * groups, states),
            conv_bc.reshape(-1, 2 * groups, states),
            dt_bias.reshape(1, heads),
            a_log.reshape(1, heads),
            d_skip.reshape(1, heads),
        ),
        [
            pltpu.VMEM((groups, wide), F32),
            pltpu.VMEM((groups, wide), F32),
            pltpu.VMEM((2 * groups, states), F32),
        ],
    )
    mixed = share_kv(mixed, kv)
    joined = run(
        functools.partial(mix_out_body, seqs, tp),
        f32(seqs, span),
        (*mixed, w_join, first),
        [pltpu.VMEM((2 * seqs, flat), F32)],
    )
    second = share_chip((joined + swap_tp(joined)).astype(BF16))
    gate_two = turned_layer(gate, 1)
    up_two = turned_layer(up, 1)
    keep, give, base = run(
        functools.partial(second_body, seqs),
        [f32(seqs, 4 * width), f32(seqs, 4 * width), f32(seqs, width)],
        (*second, rows, gate_two, up_two, down),
        [pltpu.VMEM((kv * tp, seqs, width), F32), pltpu.VMEM((kv * tp, seqs, width), F32)],
    )
    total = keep + swap_tp(give)
    sent = total.astype(BF16)
    far = swap_far(sent[:, : 2 * width])
    near = swap_near(sent[:, 2 * width : 3 * width])
    passed = swap_tp(far[:, width:]).astype(F32)
    rest = total[:, 3 * width :] + far[:, :width].astype(F32) + near.astype(F32) + passed
    return (base + 0.5 * rest).astype(BF16)


def normalize(rows, gain):
    values = rows.astype(jnp.float32)
    scale = lax.rsqrt(jnp.mean(values * values, axis=1, keepdims=True) + EPS)
    return (values * scale * gain.astype(jnp.float32).reshape(1, -1)).astype(jnp.bfloat16)


def feed_forward(normed, w_gate, w_up, w_down):
    gate = jnp.dot(normed, w_gate, preferred_element_type=jnp.float32)
    upper = jnp.dot(normed, w_up, preferred_element_type=jnp.float32)
    hidden = (jax.nn.silu(gate) * upper).astype(jnp.bfloat16)
    return jnp.dot(hidden, w_down, preferred_element_type=jnp.float32)


def add_half(base, sums):
    return (base.astype(jnp.float32) + 0.5 * sums).astype(jnp.bfloat16)


def ffn_totals(partial_value):
    return lax.psum(partial_value, ("kv", "tp"))


def short_conv(history, newest, taps):
    window = jnp.concatenate(
        [history.astype(jnp.float32), newest.astype(jnp.float32)[:, None]], axis=1
    )
    return jax.nn.silu(jnp.sum(window * taps.astype(jnp.float32)[None], axis=1))


def state_step(
    xs_new,
    zeta,
    bc_new,
    dt_raw,
    conv_x,
    conv_bc,
    ssm_state,
    conv_wx,
    conv_wbc,
    dt_bias,
    a_log,
    d_skip,
):
    xconv = short_conv(conv_x, xs_new, conv_wx)
    bconv = short_conv(conv_bc, bc_new, conv_wbc)
    heads = xconv.shape[1]
    groups = bconv.shape[2]
    bmat = jnp.repeat(bconv[:, 0], heads // groups, axis=1)
    cmat = jnp.repeat(bconv[:, 1], heads // groups, axis=1)
    step_size = jax.nn.softplus(dt_raw + dt_bias[None, :])
    decay = jnp.exp(-step_size * jnp.exp(a_log)[None, :])
    updated = (
        decay[:, :, None, None] * ssm_state
        + (step_size[:, :, None] * xconv)[..., None] * bmat[:, :, None, :]
    )
    mixed = (
        jnp.einsum("shpn,shn->shp", updated, cmat, precision=lax.Precision.HIGHEST)
        + d_skip[None, :, None] * xconv
    )
    return (mixed * jax.nn.silu(zeta.astype(jnp.float32))).astype(jnp.bfloat16)


def group_terms(slab, w_bc, w_dt):
    span = slab.shape[1]
    flat_bc = w_bc.reshape(span, -1)
    bc_part = jnp.dot(slab, flat_bc, preferred_element_type=jnp.float32)
    dt_part = jnp.dot(slab, w_dt, preferred_element_type=jnp.float32)
    return (
        lax.psum_scatter(bc_part, "kv", scatter_dimension=0, tiled=True),
        lax.psum_scatter(dt_part, "kv", scatter_dimension=0, tiled=True),
    )


def mix_partial(
    normed,
    w_x,
    w_z,
    w_bc,
    w_dt,
    dt_bias,
    a_log,
    d_skip,
    conv_wx,
    conv_wbc,
    conv_x,
    conv_bc,
    ssm_state,
    w_out,
):
    rows = normed.shape[0]
    local_heads = w_x.shape[1]
    half = w_x.shape[2]
    xs_part = (
        jnp.dot(normed, w_x.reshape(normed.shape[1], -1), preferred_element_type=jnp.float32)
        .astype(jnp.bfloat16)
        .reshape(rows, local_heads, half)
    )
    zeta_part = (
        jnp.dot(normed, w_z.reshape(normed.shape[1], -1), preferred_element_type=jnp.float32)
        .astype(jnp.bfloat16)
        .reshape(rows, local_heads, half)
    )
    xs_new, zeta = (
        lax.all_to_all(xs_part, "kv", split_axis=0, concat_axis=1, tiled=True),
        lax.all_to_all(zeta_part, "kv", split_axis=0, concat_axis=1, tiled=True),
    )
    span = w_bc.shape[0]
    slab = lax.dynamic_slice_in_dim(normed, lax.axis_index("kv") * span, span, 1)
    bc_sum, dt_raw = group_terms(slab, w_bc, w_dt)
    bc_new = bc_sum.astype(jnp.bfloat16).reshape((bc_sum.shape[0],) + w_bc.shape[1:])
    mixed = state_step(
        xs_new,
        zeta,
        bc_new,
        dt_raw,
        conv_x,
        conv_bc,
        ssm_state,
        conv_wx,
        conv_wbc,
        dt_bias,
        a_log,
        d_skip,
    )
    flat_out = w_out.reshape(-1, w_out.shape[2])
    piece = lax.all_gather(mixed, "kv", axis=0, tiled=True)
    return jnp.dot(piece.reshape(piece.shape[0], -1), flat_out, preferred_element_type=jnp.float32)


def per_device(
    resid,
    norm_gain,
    ffn_gate,
    ffn_up,
    ffn_down,
    w_x,
    w_z,
    w_bc,
    w_dt,
    dt_bias,
    a_log,
    d_skip,
    conv_wx,
    conv_wbc,
    conv_x,
    conv_bc,
    ssm_state,
    w_out,
):
    mixer_args = (
        w_x,
        w_z,
        w_bc,
        w_dt,
        dt_bias,
        a_log,
        d_skip,
        conv_wx,
        conv_wbc,
        conv_x,
        conv_bc,
        ssm_state,
        w_out,
    )
    rows, gains = (
        lax.all_gather(resid, ("kv", "tp"), axis=1, tiled=True),
        lax.all_gather(norm_gain, ("kv", "tp"), axis=1, tiled=True),
    )
    first = add_half(
        rows,
        ffn_totals(feed_forward(normalize(rows, gains[0]), ffn_gate[0], ffn_up[0], ffn_down[0])),
    )
    partial_value = mix_partial(normalize(first, gains[1]), *mixer_args)
    span = partial_value.shape[1]
    block = lax.dynamic_slice_in_dim(first, lax.axis_index("kv") * span, span, 1)
    joined = (block.astype(jnp.float32) + lax.psum(partial_value, "tp")).astype(jnp.bfloat16)
    second = lax.all_gather(joined, "kv", axis=1, tiled=True)
    final = add_half(
        second,
        ffn_totals(feed_forward(normalize(second, gains[2]), ffn_gate[1], ffn_up[1], ffn_down[1])),
    )
    width = resid.shape[1]
    return lax.dynamic_slice_in_dim(final, lax.axis_index(("kv", "tp")) * width, width, 1)


def solution(mesh):
    placed = (
        P("dp", ("kv", "tp")),
        P(None, ("kv", "tp")),
        P(None, None, ("kv", "tp")),
        P(None, None, ("kv", "tp")),
        P(None, ("kv", "tp"), None),
        P(None, "kv", "tp"),
        P(None, "kv", "tp"),
        P("kv", None, None, None),
        P("kv", None),
        P(),
        P(),
        P(),
        P(None, None, "tp"),
        P(),
        P(("dp", "kv"), None, None, "tp"),
        P(("dp", "kv"), None, None, None, None),
        P(("dp", "kv"), None, "tp", None),
        P(None, "tp", "kv"),
    )
    kv, tp = mesh.shape["kv"], mesh.shape["tp"]
    small = (kv, tp) == (4, 2)
    return jax.shard_map(
        functools.partial(small_mesh, kv, tp) if small else per_device,
        mesh=mesh,
        in_specs=placed,
        out_specs=P("dp", ("kv", "tp")),
        check_vma=False,
    )
```
